512 devices in a mesh: sp: 32 (over z, core), tp: 16 (over y, x).
Axes of the slice: x: 4, y: 4, z: 16, core: 2. Of those that a mesh axis runs over, the one named last changes fastest.
Arguments:
- skip_path_vectors: bfloat16 [8192, 2048], P('sp'), may hold values from -10 to 10
- asker_raw_scores: bfloat16 [8192, 2048], P('sp', 'tp'), may hold values from -6 to 6
- retain_raw_scores: bfloat16 [8192, 2048], P('sp', 'tp'), may hold values from -5.5 to 5.5
- memory_write_entries: bfloat16 [8192, 2048], P('sp', 'tp'), may hold values from -6 to 6
- emit_switch_scores: bfloat16 [8192, 2048], P('sp', 'tp'), may hold values from -6 to 6
- retain_minimum_share: float32 [2048], P('tp'), may hold values from 0.88 to 0.99997559
- extra_shrink_rate: float32 [16, 8192], P('tp', 'sp'), may hold values from -0.7 to 0
- lane_rescale_factor: float32 [128], replicated, may hold values from 0.1 to 1.9
- emit_projection_array: bfloat16 [2048, 2048], P('tp'), may hold values from -0.1875 to 0.1875
- specialist_rescale_factor: float32 [2048], replicated, may hold values from 0.1 to 1.9
- specialist_switch_proj: bfloat16 [32, 2048, 4096], P('sp', None, 'tp'), may hold values from -0.125 to 0.125
- specialist_raise_proj: bfloat16 [32, 2048, 4096], P('sp', None, 'tp'), may hold values from -0.125 to 0.125
- specialist_lower_proj: bfloat16 [32, 4096, 2048], P('sp', 'tp'), may hold values from -0.375 to 0.375
- specialist_choice_ids: int32 [8192, 2], P('sp'), may hold values from 0 to 31, all different within a row; in each aligned block of 256 rows (0 to 255, 256 to 511, ...) at most 24 rows name the same one
- cluster_chance: float32 [8192], P('sp'), may hold values from 0.1 to 0.6
- specialist_duo_scores: float32 [8192, 2], P('sp'), may hold values from -2 to 2
Outputs:
- mixed_out: bfloat16 [8192, 2048], P('sp', 'tp')
The draws below stay inside these ranges and needn't reach their ends.
Inputs may be any that keep to these rules, and one draw needn't show every extreme that they name: `specialist_choice_ids`: in each aligned block of 256 rows (the rows of one index of sp) no expert is named by more than 24 rows, a bound that some block reaches; the 2 ids of a row differ.
All inputs are finite; a program needn't handle non-finite values.
Results may differ from the reference program's by a relative error of at most 0.02.
Values may be sent and summed in bfloat16 or wider, within the bound.
A program may use at most 64 MiB of HBM per device.

```python
import math
import jax
import jax.numpy as jnp
import numpy as np
from jax import lax

D = 2048
SCAN_LANE_COUNT = 16
KEY_WIDTH_SIZE = 128
FFE = 4096
TOPK = 2
TOK_SP = 256
HG_W = 2048
EXPERTS = 32
SEQ = 8192
CAP = 24
N_SP = 32
N_TP = 16


def draw_skip_path_vectors(key, part):
    noise_key, row_key = jax.random.split(key)
    columns = jnp.arange(D, dtype=jnp.float32) / D
    noise = jnp.clip(jax.random.normal(noise_key, (SEQ, D), jnp.float32), -3.0, 3.0)
    col_scale = 10.0 ** (columns - 0.5)
    row_scale = 0.3 * jnp.exp(jax.random.uniform(row_key, (SEQ,), jnp.float32, math.log(0.3), math.log(3.0)))
    return (noise * row_scale[:, None] * col_scale[None, :]).astype(jnp.bfloat16)


def draw_retain_raw_scores(key, part):
    noise_key, shift_key = jax.random.split(key)
    blocks = SEQ // TOK_SP
    noise = jnp.clip(jax.random.normal(noise_key, (SEQ, HG_W), jnp.float32), -4.0, 4.0)
    shifts = jax.random.uniform(shift_key, (blocks, 1, 1), jnp.float32, -1.0, 1.0)
    return (noise.reshape(blocks, TOK_SP, HG_W) + shifts).reshape(SEQ, HG_W).astype(jnp.bfloat16)


def draw_retain_minimum_share(key, part):
    pick_key, slow_key, fast_key = jax.random.split(key, 3)
    slow_head = jax.random.randint(pick_key, (SCAN_LANE_COUNT,), 0, 2) > 0
    slow_gap = jnp.exp(jax.random.uniform(slow_key, (SCAN_LANE_COUNT, KEY_WIDTH_SIZE), jnp.float32, math.log(0.2), math.log(1.2))) / SEQ
    fast_gap = jnp.exp(jax.random.uniform(fast_key, (SCAN_LANE_COUNT, KEY_WIDTH_SIZE), jnp.float32, math.log(0.04), math.log(0.12)))
    gap = jnp.where(slow_head[:, None], slow_gap, fast_gap)
    return (1.0 - gap).reshape(HG_W).astype(jnp.float32)


def draw_extra_shrink_rate(key, part):
    where_key, size_key = jax.random.split(key)
    spots = jax.random.randint(where_key, (3,), 0, SEQ)
    strength = jnp.log(jax.random.uniform(size_key, (SCAN_LANE_COUNT, 3), jnp.float32, 0.5, 0.8))
    places = jnp.arange(SEQ)[None, None, :] == spots[None, :, None]
    return jnp.sum(jnp.where(places, strength[:, :, None], 0.0), axis=1).astype(jnp.float32)


def with_spikes(values, rng, source, target, blocks, factor):
    def block_of(position):
        return (jnp.arange(values.shape[position]) // (values.shape[position] // blocks)).reshape((-1,) + (1,) * (values.ndim - 1 - position))

    near = jax.random.permutation(rng, blocks)[block_of(target)]
    other_side = (block_of(target) + blocks // 2) % blocks
    return jnp.where((block_of(source) == near) | (block_of(source) == other_side), factor * values, values)


def steps_of(stream_key, dims, cuts, low, largest):
    gain, own = 1.0, jax.random.fold_in(stream_key, 6)
    for axis_at, parts in cuts:
        steps = jnp.exp(jax.random.uniform(jax.random.fold_in(own, axis_at), (parts,), jnp.float32, low / len(cuts), largest / len(cuts)))
        gain = gain * jnp.repeat(steps, dims[axis_at] // parts).reshape([-1 if axis == axis_at else 1 for axis in range(len(dims))])
    return gain


def routed_block(rng, own, number, rows, count, top, limit, skew):
    ranking = jax.random.permutation(rng, count)
    crowded, ordinary = shares(count, rows * top, limit, skew, True), shares(count, rows * top, limit, skew, False)
    places = jnp.arange(count)

    def named(sizes, rotation):
        used = int((sizes > 0).sum())
        fixed = max(1, used // 4)
        shifted = fixed + (places - fixed + rotation * (used - fixed)) % max(1, count - fixed)
        return jnp.zeros((count,), jnp.int32).at[ranking[jnp.where(places < fixed, places, shifted)]].set(jnp.asarray(sizes, jnp.int32))

    sizes = jnp.where(number % 4 == 0, named(crowded, number // 4), named(ordinary, number - number // 4 - 1))
    mixed = jax.random.permutation(jax.random.fold_in(own, 3), count)
    source_of, taker = mixed[0:count // 2 * 2:2], mixed[1:count // 2 * 2:2]
    margin = jnp.minimum(sizes[source_of] - 1, limit - sizes[taker]) // 2
    margin = jnp.where((source_of == ranking[0]) | (taker == ranking[0]) | (sizes[taker] == 0), 0, jnp.maximum(margin, 0))
    shifted = jax.random.randint(jax.random.fold_in(own, 4), (count // 2,), 0, 1 << 20) % (margin + 1)
    sizes = sizes.at[source_of].add(-shifted).at[taker].add(shifted)
    labels = jnp.searchsorted(jnp.cumsum(sizes), jnp.arange(rows * top), side="right").astype(jnp.int32)
    grid = labels.reshape(top, rows).T
    grid = grid[jax.random.permutation(jax.random.fold_in(own, 1), rows)]
    rotation = jax.random.randint(jax.random.fold_in(own, 2), (rows, 1), 0, top)
    return jnp.take_along_axis(grid, (jnp.arange(top)[None, :] + rotation) % top, axis=1)


def shares(amount, total, bound, slope, full):
    weights = [(1 << 20) // math.isqrt(standing ** slope) + 1 for standing in range(1, amount + 1)]
    largest = bound if full else min(bound, max(-(-total // amount), total * weights[0] // sum(weights)))
    least = 1 if total - largest >= amount - 1 else 0
    holding, surplus = [largest] + [least] * (amount - 1), total - largest - least * (amount - 1)
    while surplus > 0:
        candidates = [i for i in range(1, amount) if holding[i] < largest] or [i for i in range(1, amount) if holding[i] < bound]
        mass, remaining = sum([weights[i] for i in candidates]), surplus
        for i in candidates:
            addition = min(bound - holding[i], max(1, remaining * weights[i] // mass), surplus)
            holding[i] = holding[i] + addition
            surplus = surplus - addition
    return np.array(holding)


def scatter_about(rng, shape, width, most, shards=(), held_as=jnp.bfloat16):
    loudness = steps_of(rng, shape, shards, -0.22, 0.18) if shards else 1.0
    entries = jax.random.normal(rng, shape, jnp.float32) * width * loudness
    return jnp.minimum(jnp.maximum(entries, -most), most).astype(held_as)


def bell_draw_with(rng, shape, width, limit, pieces, heavy, kind=jnp.bfloat16):
    values = width * jax.random.normal(rng, shape, jnp.float32)
    if pieces:
        values = values * steps_of(rng, shape, pieces, -0.22, 0.18)
    return jnp.clip(with_spikes(values, jax.random.fold_in(rng, 3), *heavy), -limit, limit).astype(kind)


def setup_inputs(seed: int = 0) -> dict:
    streams_of = jax.random.split(jax.random.key(seed), 17)
    skip_path_vectors = draw_skip_path_vectors(jax.random.fold_in(streams_of[16], 71), 0)
    asker_raw_scores = scatter_about(streams_of[1], (SEQ, HG_W), 1.0, 6.0, ((0, 32), (1, 16)))
    retain_raw_scores = draw_retain_raw_scores(jax.random.fold_in(streams_of[16], 71), 0)
    memory_write_entries = scatter_about(streams_of[3], (SEQ, HG_W), 1.0, 6.0, ((0, 32), (1, 16)))
    emit_switch_scores = scatter_about(streams_of[4], (SEQ, HG_W), 1.0, 6.0, ((0, 32), (1, 16)))
    retain_minimum_share = draw_retain_minimum_share(jax.random.fold_in(streams_of[16], 71), 0)
    extra_shrink_rate = draw_extra_shrink_rate(jax.random.fold_in(streams_of[16], 71), 0)
    lane_rescale_factor = jnp.clip(1.0 + 0.18 * jax.random.normal(streams_of[7], (KEY_WIDTH_SIZE,), jnp.float32), 0.1, 1.9)
    emit_projection_array = bell_draw_with(streams_of[8], (HG_W, D), HG_W ** -0.5, 0.1875, ((0, 16),), (0, 1, 16, 2.0))
    specialist_rescale_factor = jnp.clip(1.0 + 0.18 * jax.random.normal(streams_of[9], (D,), jnp.float32), 0.1, 1.9)
    specialist_switch_proj = scatter_about(streams_of[10], (EXPERTS, D, FFE), D ** -0.5, 0.125, ((0, 32), (2, 16)))
    specialist_raise_proj = scatter_about(streams_of[11], (EXPERTS, D, FFE), D ** -0.5, 0.125, ((0, 32), (2, 16)))
    specialist_lower_proj = bell_draw_with(streams_of[12], (EXPERTS, FFE, D), (FFE // 8) ** -0.5, 0.375, ((0, 32), (1, 16)), (1, 2, 16, 2.0))
    specialist_choice_ids_keys = jax.random.split(jax.random.fold_in(streams_of[13], 1), SEQ // TOK_SP)
    specialist_choice_ids_turns = jax.random.permutation(jax.random.fold_in(streams_of[13], 3), SEQ // TOK_SP)
    specialist_choice_ids = jax.vmap(lambda own, number: routed_block(jax.random.fold_in(streams_of[13], 2), own, number, TOK_SP, EXPERTS, TOPK, CAP, 2))(specialist_choice_ids_keys, specialist_choice_ids_turns).reshape((SEQ, TOPK))
    cluster_chance = jnp.clip(0.1 + 0.5 * jax.random.uniform(streams_of[14], (SEQ,), jnp.float32) ** steps_of(streams_of[14], (SEQ,), ((0, 32),), -0.2, 0.2), 0.1, 0.6)
    specialist_duo_scores = scatter_about(streams_of[15], (SEQ, TOPK), 0.5, 2.0, ((0, 32),), jnp.float32)
    return dict(skip_path_vectors=skip_path_vectors, asker_raw_scores=asker_raw_scores, retain_raw_scores=retain_raw_scores, memory_write_entries=memory_write_entries, emit_switch_scores=emit_switch_scores, retain_minimum_share=retain_minimum_share, extra_shrink_rate=extra_shrink_rate, lane_rescale_factor=lane_rescale_factor, emit_projection_array=emit_projection_array, specialist_rescale_factor=specialist_rescale_factor, specialist_switch_proj=specialist_switch_proj, specialist_raise_proj=specialist_raise_proj, specialist_lower_proj=specialist_lower_proj, specialist_choice_ids=specialist_choice_ids, cluster_chance=cluster_chance, specialist_duo_scores=specialist_duo_scores)


EPS = 1e-06
PRECISE = lax.Precision.HIGHEST

def recurrence(queries, key_rows, values, shrink_log_rate):
    token_count_total = queries.shape[0]
    span_len = 64
    span_count = token_count_total // span_len
    causal = (jnp.arange(span_len)[:, None] >= jnp.arange(span_len)[None, :])[:, :, None, None]

    def advance(carried, inputs):
        query_span, key_span, value_span, decay_span = inputs
        cumulative = jnp.cumsum(decay_span, axis=0)
        spread = cumulative[:, None] - cumulative[None, :]
        factor = jnp.exp(jnp.where(causal, spread, -jnp.inf))
        scores = jnp.einsum('thd,shd,tshd->hts', query_span, key_span, factor, precision=PRECISE)
        inside = jnp.einsum('hts,shv->thv', scores, value_span, precision=PRECISE)
        outside = jnp.einsum('thd,hdv->thv', query_span * jnp.exp(cumulative), carried, precision=PRECISE)
        final_cum = cumulative[-1]
        written = jnp.einsum('shd,shv->hdv', key_span * jnp.exp(final_cum[None] - cumulative), value_span, precision=PRECISE)
        carried = jnp.exp(final_cum)[:, :, None] * carried + written
        return (carried, inside + outside)

    def split_spans(array):
        return array.reshape(span_count, span_len, SCAN_LANE_COUNT, KEY_WIDTH_SIZE)
    initial = jnp.zeros((SCAN_LANE_COUNT, KEY_WIDTH_SIZE, KEY_WIDTH_SIZE), jnp.float32)
    finished, output = lax.scan(advance, initial, tuple((split_spans(a) for a in (queries, key_rows, values, shrink_log_rate))))
    return output.reshape(token_count_total, SCAN_LANE_COUNT, KEY_WIDTH_SIZE)

def split_sum(left, right, groups):
    group_width = left.shape[1] // groups

    def add_group(running, group_idx):
        part_left = lax.dynamic_slice_in_dim(left, group_idx * group_width, group_width, 1)
        part_right = lax.dynamic_slice_in_dim(right, group_idx * group_width, group_width, 0)
        piece_sum = jnp.dot(part_left, part_right, preferred_element_type=jnp.float32)
        piece_sum = lax.optimization_barrier(piece_sum.astype(jnp.bfloat16)).astype(jnp.float32)
        return (running + piece_sum, None)
    zeros = jnp.zeros((left.shape[0], right.shape[1]), jnp.float32)
    total, finished = lax.scan(add_group, zeros, jnp.arange(groups, dtype=jnp.int32))
    return total

def experts_apply(normed, specialist_choice_ids, flat_weights, specialist_switch_proj, specialist_raise_proj, specialist_lower_proj):
    top_count = specialist_choice_ids.shape[1]
    flat_ids = specialist_choice_ids.reshape(-1)
    slot_limit = N_SP * CAP

    def one_expert(running, expert):
        ordering = jnp.argsort((flat_ids != expert).astype(jnp.int32), stable=True)[:slot_limit].astype(jnp.int32)
        chosen = flat_ids[ordering] == expert
        token_idx = (ordering // top_count).astype(jnp.int32)
        routed_rows = normed[token_idx]
        gate_acts = jnp.dot(routed_rows, specialist_switch_proj[expert], preferred_element_type=jnp.float32)
        up_acts = jnp.dot(routed_rows, specialist_raise_proj[expert], preferred_element_type=jnp.float32)
        hidden = (jax.nn.silu(gate_acts) * up_acts).astype(jnp.bfloat16)
        out_rows = split_sum(hidden, specialist_lower_proj[expert], N_TP).astype(jnp.bfloat16)
        scaled = jnp.where(chosen, flat_weights[ordering], 0.0)[:, None] * out_rows.astype(jnp.float32)
        return (running.at[token_idx].add(scaled), None)
    zeros = jnp.zeros(normed.shape, jnp.float32)
    total, finished = lax.scan(one_expert, zeros, jnp.arange(EXPERTS, dtype=jnp.int32))
    return total

def reference(skip_path_vectors, asker_raw_scores, retain_raw_scores, memory_write_entries, emit_switch_scores, retain_minimum_share, extra_shrink_rate, lane_rescale_factor, emit_projection_array, specialist_rescale_factor, specialist_switch_proj, specialist_raise_proj, specialist_lower_proj, specialist_choice_ids, cluster_chance, specialist_duo_scores):
    token_count_total = skip_path_vectors.shape[0]
    retain_share = retain_minimum_share + (1.0 - retain_minimum_share) * jax.nn.sigmoid(retain_raw_scores.astype(jnp.float32))
    shrink_log_rate = jnp.log(retain_share).reshape(token_count_total, SCAN_LANE_COUNT, KEY_WIDTH_SIZE) + extra_shrink_rate.T[:, :, None]
    key_rows = (1.0 - retain_share).reshape(token_count_total, SCAN_LANE_COUNT, KEY_WIDTH_SIZE)
    queries = jax.nn.silu(asker_raw_scores.astype(jnp.float32)).reshape(token_count_total, SCAN_LANE_COUNT, KEY_WIDTH_SIZE)
    values = memory_write_entries.astype(jnp.float32).reshape(token_count_total, SCAN_LANE_COUNT, KEY_WIDTH_SIZE)
    readout = recurrence(queries, key_rows, values, shrink_log_rate)
    normed_heads = readout * lax.rsqrt(lax.optimization_barrier(jnp.mean(readout * readout, axis=-1, keepdims=True)) + EPS)
    gated_out = normed_heads * lane_rescale_factor * jax.nn.silu(emit_switch_scores.astype(jnp.float32).reshape(token_count_total, SCAN_LANE_COUNT, KEY_WIDTH_SIZE))
    mixer_out = gated_out.reshape(token_count_total, SCAN_LANE_COUNT * KEY_WIDTH_SIZE).astype(jnp.bfloat16)
    resid = (skip_path_vectors.astype(jnp.float32) + split_sum(mixer_out, emit_projection_array, N_TP)).astype(jnp.bfloat16)
    wide_rows = resid.astype(jnp.float32)
    normed = (wide_rows * lax.rsqrt(lax.optimization_barrier(jnp.mean(wide_rows * wide_rows, axis=1, keepdims=True)) + EPS) * specialist_rescale_factor).astype(jnp.bfloat16)
    spread_logit = specialist_duo_scores[:, 0] - specialist_duo_scores[:, 1]
    weights = cluster_chance[:, None] * jnp.stack([jax.nn.sigmoid(spread_logit), jax.nn.sigmoid(-spread_logit)], axis=1)
    routed = experts_apply(normed, specialist_choice_ids, weights.reshape(-1), specialist_switch_proj, specialist_raise_proj, specialist_lower_proj)
    return (wide_rows + routed).astype(jnp.bfloat16)
```

```python
import functools

import jax
import jax.numpy as jnp
from jax import lax
from jax.experimental import pallas as pl
from jax.experimental.pallas import tpu as pltpu
from jax.sharding import Mesh
from jax.sharding import PartitionSpec as P

AXES = ("z", "c", "y", "x")
SP = ("z", "c")
TP = ("y", "x")
EPS = 1e-06
BF = jnp.bfloat16
F32 = jnp.float32
HIGH = lax.Precision.HIGHEST
MESH = pl.DeviceIdType.MESH
CHUNK = 4
TILE = 8


def dims_of(a, b, left, right, precision=None):
    return lax.dot_general(
        a, b, (((left,), (right,)), ((), ())), precision=precision, preferred_element_type=F32
    )


def z_steps(count):
    steps = [0]
    for far in range(1, count // 2 + 1):
        steps += [far, -far]
    return steps[:count]


def column_of(row, eye):
    return jnp.sum(jnp.where(eye, row, 0.0), axis=1, keepdims=True)


class Wire:
    def __init__(self, sends, recvs):
        self.sends, self.recvs, self.used, self.started = sends, recvs, 0, []

    def slots(self, count):
        first = self.used
        self.used += count
        return first

    def copy(self, src, dst, number, device):
        return pltpu.make_async_remote_copy(
            src_ref=src,
            dst_ref=dst,
            send_sem=self.sends.at[number],
            recv_sem=self.recvs.at[number],
            device_id=device,
            device_id_type=MESH,
        )

    def send(self, src, dst, number, device):
        copy = self.copy(src, dst, number, device)
        copy.start()
        self.started.append(copy)

    def arrived(self, dst, number, device):
        self.copy(dst, dst, number, device).wait_recv()


def semaphore_count(nz, nc, tp):
    blocks = nz * nc
    chunks = max(1, nz // CHUNK)
    return 1 + 3 + 3 + 1 + 2 * blocks + (chunks * 32 + 16 if tp > 1 else 0)


def kernel(
    sizes,
    asker,
    retain,
    entries,
    emit,
    least,
    extra,
    lane_gain,
    row_gain,
    ids,
    chance,
    duo,
    skip_hbm,
    project_hbm,
    switch_hbm,
    raise_hbm,
    lower_hbm,
    out,
    skip,
    project,
    switch,
    raised,
    lower,
    state_own,
    state_first,
    half_out,
    half_in,
    near,
    far,
    back_out,
    back_in,
    prefix,
    query_hat,
    inside,
    gates,
    select_in,
    select_out,
    route,
    mix_part,
    mix_one,
    mix_two,
    mix_sum,
    mix_three,
    mix_four,
    slots,
    rows,
    normed,
    part,
    red_one,
    red_two,
    red_sum,
    red_three,
    red_four,
    finished,
    returned,
    local_sems,
    sends,
    recvs,
):
    nz, nc, ny, nx, tokens, cap = sizes
    tp = ny * nx
    groups = nz // 4
    half = tokens // 2
    z, c, y, x = (lax.axis_index(a) for a in AXES)
    me_sp = z * nc + c
    wire = Wire(sends, recvs)
    steps = z_steps(nz)
    chunks = nz // CHUNK

    def device(dz=0, dc=0, dy=0, dx=0):
        return (
            lax.rem(z + (dz + nz), nz),
            lax.rem(c + dc, nc),
            lax.rem(y + (dy + ny), ny),
            lax.rem(x + (dx + nx), nx),
        )

    partner = device(dc=1)
    barrier = pltpu.get_barrier_semaphore()
    peers = [device(dz=dz, dc=dc) for dz in steps for dc in range(nc) if (dz, dc) != (0, 0)]
    if tp > 1:
        peers += [device(dy=1), device(dy=-1), device(dx=1), device(dx=-1)]
    for peer in peers:
        pl.semaphore_signal(barrier, inc=1, device_id=peer, device_id_type=MESH)

    my_cols = pl.ds(pl.multiple_of((y * nx + x) * 128, 128), 128)
    loads = [
        pltpu.make_async_copy(src, dst, local_sems.at[i])
        for i, (src, dst) in enumerate(
            [
                (project_hbm, project),
                (skip_hbm.at[:, my_cols], skip),
                (switch_hbm, switch),
                (raise_hbm, raised),
                (lower_hbm, lower),
            ]
        )
    ]
    for load in loads:
        load.start()

    spots = lax.broadcasted_iota(jnp.int32, (half, half), 0)
    other = lax.broadcasted_iota(jnp.int32, (half, half), 1)
    causal = spots >= other
    causal_ones = jnp.where(causal, 1.0, 0.0).astype(F32)
    eye_half = spots == other

    def decays(b):
        mine = pl.ds(b * half, half)
        floor = least[...]
        share = floor + (1.0 - floor) * jax.nn.sigmoid(retain[mine, :].astype(F32))
        logs = jnp.log(share) + column_of(extra[:, b * half : (b + 1) * half], eye_half)
        total = jnp.dot(causal_ones, logs, precision=HIGH, preferred_element_type=F32)
        return total, 1.0 - share

    states, lasts, kept = [], [], []
    for b in range(2):
        total, keys = decays(b)
        last = total[half - 1 : half, :]
        ending = keys * jnp.exp(last - total)
        values = entries[b * half : (b + 1) * half, :].astype(F32)
        states.append(dims_of(values, ending, 0, 0, HIGH))
        lasts.append(last)
        kept.append((total, keys))
    own_decay = jnp.exp(lasts[0] + lasts[1])
    state_first[...] = states[0]
    state_own[...] = jnp.exp(lasts[1]) * states[0] + states[1]

    tail_row = lax.broadcasted_iota(jnp.int32, (16, 128), 0)

    def pack(ref, value, decay):
        top = decay.astype(BF)
        low = (decay - top.astype(F32)).astype(BF)
        ref[0:64, :] = value.astype(BF)
        tail = jnp.where(
            tail_row == 0, top.astype(F32), jnp.where(tail_row == 1, low.astype(F32), 0.0)
        )
        ref[64:80, :] = tail.astype(BF)

    def unpack(ref):
        tail = ref[64:80, :].astype(F32)
        return ref[0:64, :].astype(F32), tail[0:1, :] + tail[1:2, :]

    first_core = c == 0
    mine_half = jnp.where(first_core, state_own[0:64, :], state_own[64:128, :])
    theirs_half = jnp.where(first_core, state_own[64:128, :], state_own[0:64, :])
    pack(half_out, theirs_half, own_decay)

    pl.semaphore_wait(barrier, len(peers))

    n_half = wire.slots(1)
    n_near = wire.slots(3)
    n_far = wire.slots(3)
    n_back = wire.slots(1)
    wire.send(half_out, half_in, n_half, partner)

    def score_block(b):
        total, keys = kept[b]
        mine = pl.ds(b * half, half)
        middle = total[half // 2 - 1 : half // 2, :]
        asked = jax.nn.silu(asker[mine, :].astype(F32))
        query_hat[mine, :] = asked * jnp.exp(total)
        scores = dims_of(
            asked * jnp.exp(total - middle), keys * jnp.exp(middle - total), 1, 1, HIGH
        )
        scores = jnp.where(causal, scores, 0.0)
        values = entries[mine, :].astype(F32)
        inside[mine, :] = jnp.dot(scores, values, precision=HIGH, preferred_element_type=F32)
        gates[mine, :] = lane_gain[...] * jax.nn.silu(emit[mine, :].astype(F32))

    wire.arrived(half_in, n_half, partner)
    theirs, their_decay = unpack(half_in)
    s0 = jnp.where(first_core, mine_half, theirs)
    s1 = jnp.where(first_core, theirs, mine_half)
    d0 = jnp.where(first_core, own_decay, their_decay)
    d1 = jnp.where(first_core, their_decay, own_decay)
    group, place = z // 4, lax.rem(z, 4)
    pack(near.at[place], d1 * s0 + s1, d0 * d1)

    def in_group(j):
        return (group * 4 + lax.rem(place + j, 4), c, y, x)

    for j in (1, 2, 3):
        wire.send(near.at[place], near.at[place], n_near + j - 1, in_group(j))

    score_block(0)
    score_block(1)

    for j in (1, 2, 3):
        sender = lax.rem(place + 4 - j, 4)
        wire.arrived(near.at[sender], n_near + j - 1, in_group(4 - j))
    before = jnp.zeros((64, 128), F32)
    before_decay = jnp.ones((1, 128), F32)
    total_state, total_decay = before, before_decay
    for j in range(4):
        value, decay = unpack(near.at[j])
        total_state = decay * total_state + value
        total_decay = decay * total_decay
        earlier = j < place
        before = jnp.where(earlier, decay * before + value, before)
        before_decay = jnp.where(earlier, decay * before_decay, before_decay)
    pack(far.at[group], total_state, total_decay)

    def to_group(j):
        return (lax.rem(z + 4 * j, nz), c, y, x)

    for j in range(1, groups):

        @pl.when(group + j < groups)
        def _():
            wire.copy(far.at[group], far.at[group], n_far + j - 1, to_group(j)).start()

    tok_row = lax.broadcasted_iota(jnp.int32, (tokens, tokens), 0)
    tok_col = lax.broadcasted_iota(jnp.int32, (tokens, tokens), 1)
    eye = tok_row == tok_col
    earlier_ones = jnp.where(tok_row < tok_col, 1.0, 0.0).astype(BF)
    experts = nz * nc
    expert_at = lax.broadcasted_iota(jnp.int32, (experts, tokens), 0)
    named = [jnp.where(expert_at == ids[j : j + 1, :], 1.0, 0.0).astype(F32) for j in range(2)]
    counts = jnp.dot(
        (named[0] + named[1]).astype(BF), earlier_ones, preferred_element_type=F32
    )
    slot_rows = [
        ids[j : j + 1, :].astype(F32) * cap + jnp.sum(counts * named[j], axis=0, keepdims=True)
        for j in range(2)
    ]
    slot_at = lax.broadcasted_iota(jnp.int32, (experts * cap, tokens), 0).astype(F32)
    select_in[...] = jnp.where(
        slot_at == slot_rows[0], 1.0, jnp.where(slot_at == slot_rows[1], 1.0, 0.0)
    ).astype(BF)
    slot_along = lax.broadcasted_iota(jnp.int32, (tokens, experts * cap), 1).astype(F32)
    spread = duo[0:1, :] - duo[1:2, :]
    for j in range(2):
        select_out[j] = jnp.where(
            slot_along == column_of(slot_rows[j], eye), 1.0, 0.0
        ).astype(BF)
        weight = chance[...] * jax.nn.sigmoid(spread if j == 0 else -spread)
        route[j] = jnp.broadcast_to(column_of(weight, eye), (tokens, 128))

    prefix[...] = jnp.zeros((64, 128), F32)
    for j in range(groups - 1):

        @pl.when(j < group)
        def _():
            sender = j
            number = n_far + group - 1 - j
            wire.arrived(far.at[sender], number, to_group(0))
            value, decay = unpack(far.at[sender])
            prefix[...] = decay * prefix[...] + value

    start = before_decay * prefix[...] + before
    after_first = d0 * start + s0
    back_out[...] = jnp.where(first_core, after_first, start).astype(BF)
    wire.send(back_out, back_in, n_back, partner)
    own_start = jnp.where(first_core, start, after_first)
    wire.arrived(back_in, n_back, partner)
    got = back_in[...].astype(F32)
    carried = jnp.concatenate(
        [jnp.where(first_core, own_start, got), jnp.where(first_core, got, own_start)], axis=0
    )
    for j in range(1, groups):

        @pl.when(group + j < groups)
        def _():
            wire.copy(far.at[group], far.at[group], n_far + j - 1, to_group(j)).wait_send()

    second = jnp.exp(lasts[0]) * carried + state_first[...]
    loads[0].wait()
    for b, state in enumerate((carried, second)):
        mine = pl.ds(b * half, half)
        readout = inside[mine, :] + dims_of(query_hat[mine, :], state, 1, 1, HIGH)
        mean = jnp.mean(readout * readout, axis=1, keepdims=True)
        mixed = (readout * lax.rsqrt(mean + EPS) * gates[mine, :]).astype(BF)
        for t in range(0, tp, 2):
            wide = jnp.dot(
                mixed, project[:, t * 128 : (t + 2) * 128], preferred_element_type=F32
            )
            for u in range(t, min(t + 2, tp)):
                mix_part[u // nx, u % nx, b] = (
                    wide[:, (u - t) * 128 : (u - t + 1) * 128]
                    .reshape(2, half // 2, 128)
                    .astype(BF)
                )

    class Reduce:
        def __init__(self, source, lo, n, one, two, total, three, four):
            self.source, self.lo, self.n = source, lo, n
            self.bufs = (one, two, total, three, four)
            self.first = wire.slots(16)

        def at(self, k, f, g):
            rest = (k, pl.ds(self.lo, self.n))
            return self.source.at[(f, g) + rest] if k == 0 else self.source.at[(g, f) + rest]

        def axes(self, k):
            f, g = (y, x) if k == 0 else (x, y)
            name_f, name_g = ("dy", "dx") if k == 0 else ("dx", "dy")
            return f, g, (lambda d: device(**{name_f: d})), (lambda d: device(**{name_g: d}))

        def number(self, k, step, way):
            return self.first + k * 8 + step * 2 + way

        def step_one(self):
            one = self.bufs[0]
            for k in range(2):
                f, g, to_f, to_g = self.axes(k)
                across = lax.rem(f + 2, 4)
                for way, delta in ((0, 1), (1, -1)):
                    wire.send(
                        self.at(k, across, pl.ds(2 * way, 2)),
                        one.at[k, way],
                        self.number(k, 0, way),
                        to_f(delta),
                    )

        def step_two(self):
            one, two = self.bufs[0], self.bufs[1]
            for k in range(2):
                f, g, to_f, to_g = self.axes(k)
                for way, delta in ((0, 1), (1, -1)):
                    wire.arrived(one.at[k, way], self.number(k, 0, way), to_f(-delta))
                    mine = self.at(k, lax.rem(f + delta + 4, 4), pl.ds(2 * way, 2))
                    mine[...] = (mine[...].astype(F32) + one[k, way].astype(F32)).astype(BF)
            for k in range(2):
                f, g, to_f, to_g = self.axes(k)
                for way, delta in ((0, 1), (1, -1)):
                    wire.send(
                        self.at(k, lax.rem(f + delta + 4, 4), pl.ds(0, 4)),
                        two.at[k, way],
                        self.number(k, 1, way),
                        to_f(delta),
                    )

        def step_three(self):
            two, total, three = self.bufs[1], self.bufs[2], self.bufs[3]
            h = self.n // 2
            for k in range(2):
                f, g, to_f, to_g = self.axes(k)
                for way, delta in ((0, 1), (1, -1)):
                    wire.arrived(two.at[k, way], self.number(k, 1, way), to_f(-delta))
                total[k] = (
                    self.at(k, f, pl.ds(0, 4))[...].astype(F32)
                    + two[k, 0].astype(F32)
                    + two[k, 1].astype(F32)
                ).astype(BF)
            for k in range(2):
                f, g, to_f, to_g = self.axes(k)
                for way, delta in ((0, 1), (1, -1)):
                    wire.send(
                        total.at[k, lax.rem(g + 2, 4), pl.ds(way * h, h)],
                        three.at[k, way],
                        self.number(k, 2, way),
                        to_g(delta),
                    )

        def step_four(self):
            total, three, four = self.bufs[2], self.bufs[3], self.bufs[4]
            h = self.n // 2
            for k in range(2):
                f, g, to_f, to_g = self.axes(k)
                for way, delta in ((0, 1), (1, -1)):
                    wire.arrived(three.at[k, way], self.number(k, 2, way), to_g(-delta))
                    mine = total.at[k, lax.rem(g + delta + 4, 4), pl.ds(way * h, h)]
                    mine[...] = (mine[...].astype(F32) + three[k, way].astype(F32)).astype(BF)
            for k in range(2):
                f, g, to_f, to_g = self.axes(k)
                for way, delta in ((0, 1), (1, -1)):
                    wire.send(
                        total.at[k, lax.rem(g + delta + 4, 4)],
                        four.at[k, way],
                        self.number(k, 3, way),
                        to_g(delta),
                    )

        def result(self, k):
            two, four = self.bufs[1], self.bufs[4]
            f, g, to_f, to_g = self.axes(k)
            for way, delta in ((0, 1), (1, -1)):
                wire.arrived(four.at[k, way], self.number(k, 3, way), to_g(-delta))
            return (
                self.at(k, f, g)[...].astype(F32)
                + two[k, 0, g].astype(F32)
                + two[k, 1, g].astype(F32)
                + four[k, 0].astype(F32)
                + four[k, 1].astype(F32)
            )

    loads[1].wait()
    if tp > 1:
        mix = Reduce(mix_part, 0, 2, mix_one, mix_two, mix_sum, mix_three, mix_four)
        mix.step_one()
        mix.step_two()
        mix.step_three()
        mix.step_four()
        own_cols = [mix.result(k).reshape(half, 128) for k in range(2)]
    else:
        own_cols = [mix_part[0, 0, k].astype(F32).reshape(half, 128) for k in range(2)]
    for k in range(2):
        mine = pl.ds(k * half, half)
        skip[mine, :] = (skip[mine, :].astype(F32) + own_cols[k]).astype(BF)

    tiles = cap // TILE
    slots[...] = (
        jnp.dot(select_in[...], skip[...], preferred_element_type=F32)
        .reshape(experts, tiles, TILE, 128)
        .astype(BF)
    )
    rows[y, x, 0, 0] = slots[me_sp]
    n_out = wire.slots(nz * nc)
    for i, dz in enumerate(steps):
        for dc in range(nc):
            if (dz, dc) == (0, 0):
                continue
            there = device(dz=dz, dc=dc)
            wire.send(
                slots.at[there[0] * nc + there[1]],
                rows.at[y, x, dc, i],
                n_out + i * nc + dc,
                there,
            )

    class Chunk:
        def __init__(self, number):
            self.lo = number * CHUNK
            self.number = number
            if tp > 1:
                self.first = wire.slots(16)
                self.red = Reduce(
                    part,
                    self.lo,
                    CHUNK,
                    *(b.at[number] for b in (red_one, red_two, red_sum, red_three, red_four)),
                )

        def at(self, k, p, s, lo=0, n=CHUNK):
            rest = (k, pl.ds(self.lo + lo, n))
            return rows.at[(s, p) + rest] if k == 0 else rows.at[(p, s) + rest]

        def axes(self, k):
            p, s = (x, y) if k == 0 else (y, x)
            name_p, name_s = ("dx", "dy") if k == 0 else ("dy", "dx")
            return p, s, (lambda d: device(**{name_p: d})), (lambda d: device(**{name_s: d}))

        def sem(self, k, step, way):
            return self.first + k * 8 + step * 2 + way

        def gather_one(self):
            for i in range(self.lo, self.lo + CHUNK):
                for dc in range(nc):
                    if (steps[i], dc) != (0, 0):
                        wire.arrived(
                            rows.at[y, x, dc, i], n_out + i * nc + dc, device(dz=-steps[i], dc=dc)
                        )
            if tp == 1:
                return
            for k in range(2):
                p, s, to_p, to_s = self.axes(k)
                for way, delta in ((0, 1), (1, -1)):
                    mine = self.at(k, p, s)
                    wire.send(mine, mine, self.sem(k, 0, way), to_p(delta))

        def gather_two(self):
            h = CHUNK // 2
            for k in range(2 if tp > 1 else 0):
                p, s, to_p, to_s = self.axes(k)
                for way, delta in ((0, 1), (1, -1)):
                    came = lax.rem(p - delta + 4, 4)
                    wire.arrived(self.at(k, came, s), self.sem(k, 0, way), to_p(-delta))
                    onward = self.at(k, came, s, way * h, h)
                    wire.send(onward, onward, self.sem(k, 1, way), to_p(delta))

        def gather_three(self):
            h = CHUNK // 2
            for k in range(2 if tp > 1 else 0):
                p, s, to_p, to_s = self.axes(k)
                across = lax.rem(p + 2, 4)
                for way, delta in ((0, 1), (1, -1)):
                    wire.arrived(
                        self.at(k, across, s, way * h, h), self.sem(k, 1, way), to_p(-delta)
                    )
                mine = self.at(k, pl.ds(0, 4), s)
                for way, delta in ((0, 1), (1, -1)):
                    wire.send(mine, mine, self.sem(k, 2, way), to_s(delta))

        def gather_four(self):
            for k in range(2 if tp > 1 else 0):
                p, s, to_p, to_s = self.axes(k)
                for way, delta in ((0, 1), (1, -1)):
                    came = lax.rem(s - delta + 4, 4)
                    wire.arrived(
                        self.at(k, pl.ds(0, 4), came), self.sem(k, 2, way), to_s(-delta)
                    )
                    onward = self.at(k, pl.ds(2 * way, 2), came)
                    wire.send(onward, onward, self.sem(k, 3, way), to_s(delta))

        def experts(self):
            for k in range(2 if tp > 1 else 0):
                p, s, to_p, to_s = self.axes(k)
                across = lax.rem(s + 2, 4)
                for way, delta in ((0, 1), (1, -1)):
                    wire.arrived(
                        self.at(k, pl.ds(2 * way, 2), across), self.sem(k, 3, way), to_s(-delta)
                    )
            span = pl.ds(self.lo, CHUNK)
            count = nc * CHUNK * cap
            squares = jnp.zeros((count, 128), F32)
            for t in range(tp):
                wide = rows[t // nx, t % nx, :, span].astype(F32).reshape(count, 128)
                squares = squares + wide * wide
            scale = lax.rsqrt(jnp.sum(squares, axis=1, keepdims=True) / (tp * 128) + EPS)
            for t in range(tp):
                wide = rows[t // nx, t % nx, :, span].astype(F32).reshape(count, 128)
                cols = slice(t * 128, (t + 1) * 128)
                normed[:, cols] = (wide * scale * row_gain[:, cols]).astype(BF)
            gate_acts = jnp.dot(normed[...], switch[...], preferred_element_type=F32)
            up_acts = jnp.dot(normed[...], raised[...], preferred_element_type=F32)
            hidden = (jax.nn.silu(gate_acts) * up_acts).astype(BF)
            for t in range(0, tp, 2):
                wide = jnp.dot(
                    hidden, lower[:, t * 128 : (t + 2) * 128], preferred_element_type=F32
                )
                for u in range(t, min(t + 2, tp)):
                    part[u // nx, u % nx, :, span] = (
                        wide[:, (u - t) * 128 : (u - t + 1) * 128]
                        .reshape(nc, CHUNK, tiles, TILE, 128)
                        .astype(BF)
                    )
            if tp > 1:
                self.red.step_one()

        def sum_two(self):
            if tp > 1:
                self.red.step_two()

        def sum_three(self):
            if tp > 1:
                self.red.step_three()

        def sum_four(self):
            if tp > 1:
                self.red.step_four()

        def give_back(self):
            for k in range(2):
                if tp > 1:
                    done = self.red.result(k).astype(BF)
                else:
                    done = part[0, 0, k, pl.ds(self.lo, CHUNK)]
                finished[k, pl.ds(self.lo, CHUNK)] = done
            for i in range(self.lo, self.lo + CHUNK):
                for dc in range(nc):
                    if (steps[i], dc) == (0, 0):
                        returned[me_sp] = finished[0, 0]
                        continue
                    wire.send(
                        finished.at[dc, i],
                        returned.at[me_sp],
                        n_back_rows + i * nc + dc,
                        device(dz=-steps[i], dc=dc),
                    )

    n_back_rows = wire.slots(nz * nc)
    work = [Chunk(n) for n in range(chunks)]
    for load in loads[2:]:
        load.wait()
    order = (
        "gather_one",
        "gather_two",
        "gather_three",
        "gather_four",
        "experts",
        "sum_two",
        "sum_three",
        "sum_four",
        "give_back",
    )
    tasks = sorted((j + 2 * n, n, j) for n in range(chunks) for j in range(len(order)))
    for _, n, j in tasks:
        getattr(work[n], order[j])()

    for i, dz in enumerate(steps):
        for dc in range(nc):
            if (dz, dc) == (0, 0):
                continue
            there = device(dz=dz, dc=dc)
            wire.arrived(
                returned.at[there[0] * nc + there[1]], n_back_rows + i * nc + dc, there
            )
    got_rows = returned[...].astype(F32).reshape(experts * cap, 128).astype(BF)
    result = skip[...].astype(F32)
    for j in range(2):
        picked = jnp.dot(select_out[j], got_rows, preferred_element_type=F32)
        result = result + route[j] * picked
    out[...] = result.astype(BF)
    for copy in wire.started:
        copy.wait_send()


def layer(
    sizes,
    skip_path_vectors,
    asker_raw_scores,
    retain_raw_scores,
    memory_write_entries,
    emit_switch_scores,
    retain_minimum_share,
    extra_shrink_rate,
    lane_rescale_factor,
    emit_projection_array,
    specialist_rescale_factor,
    specialist_switch_proj,
    specialist_raise_proj,
    specialist_lower_proj,
    specialist_choice_ids,
    cluster_chance,
    specialist_duo_scores,
):
    nz, nc, ny, nx, tokens, cap = sizes
    tp = ny * nx
    width = tp * 128
    hidden = specialist_switch_proj.shape[2]
    half, experts, chunks, tiles = tokens // 2, nz * nc, nz // CHUNK, cap // TILE
    block = (tiles, TILE, 128)
    vmem, anywhere = (
        pl.BlockSpec(memory_space=pltpu.VMEM),
        pl.BlockSpec(memory_space=pl.ANY),
    )
    count = semaphore_count(nz, nc, tp)
    scratch = [
        pltpu.VMEM((tokens, 128), BF),
        pltpu.VMEM((128, width), BF),
        pltpu.VMEM((width, hidden), BF),
        pltpu.VMEM((width, hidden), BF),
        pltpu.VMEM((hidden, width), BF),
        pltpu.VMEM((128, 128), F32),
        pltpu.VMEM((128, 128), F32),
        pltpu.VMEM((80, 128), BF),
        pltpu.VMEM((80, 128), BF),
        pltpu.VMEM((4, 80, 128), BF),
        pltpu.VMEM((nz // 4, 80, 128), BF),
        pltpu.VMEM((64, 128), BF),
        pltpu.VMEM((64, 128), BF),
        pltpu.VMEM((64, 128), F32),
        pltpu.VMEM((tokens, 128), F32),
        pltpu.VMEM((tokens, 128), F32),
        pltpu.VMEM((tokens, 128), F32),
        pltpu.VMEM((experts * cap, tokens), BF),
        pltpu.VMEM((2, tokens, experts * cap), BF),
        pltpu.VMEM((2, tokens, 128), F32),
        pltpu.VMEM((ny, nx, 2, 2, half // 2, 128), BF),
        pltpu.VMEM((2, 2, 2, 2, half // 2, 128), BF),
        pltpu.VMEM((2, 2, 4, 2, half // 2, 128), BF),
        pltpu.VMEM((2, 4, 2, half // 2, 128), BF),
        pltpu.VMEM((2, 2, 1, half // 2, 128), BF),
        pltpu.VMEM((2, 2, 2, half // 2, 128), BF),
        pltpu.VMEM((experts, *block), BF),
        pltpu.VMEM((ny, nx, nc, nz, *block), BF),
        pltpu.VMEM((nc * CHUNK * cap, width), BF),
        pltpu.VMEM((ny, nx, nc, nz, *block), BF),
        pltpu.VMEM((chunks, 2, 2, 2, CHUNK, *block), BF),
        pltpu.VMEM((chunks, 2, 2, 4, CHUNK, *block), BF),
        pltpu.VMEM((chunks, 2, 4, CHUNK, *block), BF),
        pltpu.VMEM((chunks, 2, 2, CHUNK // 2, *block), BF),
        pltpu.VMEM((chunks, 2, 2, CHUNK, *block), BF),
        pltpu.VMEM((nc, nz, *block), BF),
        pltpu.VMEM((experts, *block), BF),
        pltpu.SemaphoreType.DMA((5,)),
        pltpu.SemaphoreType.DMA((count,)),
        pltpu.SemaphoreType.DMA((count,)),
    ]
    return pl.pallas_call(
        functools.partial(kernel, sizes),
        out_shape=jax.ShapeDtypeStruct((tokens, 128), BF),
        in_specs=[vmem] * 11 + [anywhere] * 5,
        out_specs=vmem,
        scratch_shapes=scratch,
        compiler_params=pltpu.CompilerParams(collective_id=0, has_side_effects=True),
    )(
        asker_raw_scores,
        retain_raw_scores,
        memory_write_entries,
        emit_switch_scores,
        retain_minimum_share.reshape(1, 128),
        extra_shrink_rate,
        lane_rescale_factor.reshape(1, 128),
        specialist_rescale_factor.reshape(1, width),
        specialist_choice_ids.T,
        cluster_chance.reshape(1, tokens),
        specialist_duo_scores.T,
        skip_path_vectors,
        emit_projection_array,
        specialist_switch_proj[0],
        specialist_raise_proj[0],
        specialist_lower_proj[0],
    )


def solution(mesh, shape=(16, 2, 4, 4), tokens=256, cap=24):
    finer = Mesh(mesh.devices.reshape(shape), AXES)
    in_specs = (
        P(SP, None),
        P(SP, TP),
        P(SP, TP),
        P(SP, TP),
        P(SP, TP),
        P(TP),
        P(TP, SP),
        P(),
        P(TP, None),
        P(),
        P(SP, None, TP),
        P(SP, None, TP),
        P(SP, TP, None),
        P(SP, None),
        P(SP),
        P(SP, None),
    )
    return jax.shard_map(
        functools.partial(layer, (*shape, tokens, cap)),
        mesh=finer,
        in_specs=in_specs,
        out_specs=P(SP, TP),
        check_vma=False,
    )
```

```python
import functools

import jax
import jax.numpy as jnp
from jax import lax
from jax.experimental import pallas as pl
from jax.experimental.pallas import tpu as pltpu
from jax.sharding import Mesh
from jax.sharding import PartitionSpec as P

AXES = ("z", "c", "y", "x")
SP = ("z", "c")
TP = ("y", "x")
EPS = 1e-06
BF = jnp.bfloat16
F32 = jnp.float32
HIGH = lax.Precision.HIGHEST
MESH = pl.DeviceIdType.MESH
CHUNK = 4
TILE = 8


def dims_of(a, b, left, right, precision=None):
    return lax.dot_general(
        a, b, (((left,), (right,)), ((), ())), precision=precision, preferred_element_type=F32
    )


def z_steps(count):
    steps = [0]
    for far in range(1, count // 2 + 1):
        steps += [far, -far]
    return steps[:count]


def column_of(row, eye):
    return jnp.sum(jnp.where(eye, row, 0.0), axis=1, keepdims=True)


class Wire:
    def __init__(self, sends, recvs):
        self.sends, self.recvs, self.used, self.started = sends, recvs, 0, []

    def slots(self, count):
        first = self.used
        self.used += count
        return first

    def copy(self, src, dst, number, device):
        return pltpu.make_async_remote_copy(
            src_ref=src,
            dst_ref=dst,
            send_sem=self.sends.at[number],
            recv_sem=self.recvs.at[number],
            device_id=device,
            device_id_type=MESH,
        )

    def send(self, src, dst, number, device):
        copy = self.copy(src, dst, number, device)
        copy.start()
        self.started.append(copy)

    def arrived(self, dst, number, device):
        self.copy(dst, dst, number, device).wait_recv()


def semaphore_count(nz, nc, tp):
    blocks = nz * nc
    chunks = max(1, nz // CHUNK)
    return 1 + 3 + 3 + 1 + 2 * blocks + (chunks * 28 + 12 if tp > 1 else 0)


def kernel(
    sizes,
    asker_hbm,
    retain_hbm,
    entries_hbm,
    emit_hbm,
    least_hbm,
    extra_hbm,
    lane_gain_hbm,
    row_gain_hbm,
    ids_hbm,
    chance_hbm,
    duo_hbm,
    skip_hbm,
    project_hbm,
    switch_hbm,
    raise_hbm,
    lower_hbm,
    out,
    asker,
    retain,
    entries,
    emit,
    least,
    extra,
    lane_gain,
    row_gain,
    ids,
    chance,
    duo,
    skip,
    project,
    switch,
    raised,
    lower,
    state_own,
    state_first,
    half_out,
    half_in,
    near,
    far,
    back_out,
    back_in,
    prefix,
    query_hat,
    inside,
    gates,
    select_in,
    select_out,
    route,
    mix_part,
    mix_one,
    mix_sum,
    mix_three,
    slots,
    rows,
    normed,
    part,
    red_one,
    red_two,
    red_sum,
    red_three,
    finished,
    returned,
    local_sems,
    sends,
    recvs,
):
    nz, nc, ny, nx, tokens, cap = sizes
    tp = ny * nx
    groups = nz // 4
    half = tokens // 2
    z, c, y, x = (lax.axis_index(a) for a in AXES)
    me_sp = z * nc + c
    wire = Wire(sends, recvs)
    steps = z_steps(nz)
    chunks = nz // CHUNK

    def device(dz=0, dc=0, dy=0, dx=0):
        return (
            lax.rem(z + (dz + nz), nz),
            lax.rem(c + dc, nc),
            lax.rem(y + (dy + ny), ny),
            lax.rem(x + (dx + nx), nx),
        )

    partner = device(dc=1)
    barrier = pltpu.get_barrier_semaphore()
    peers = [device(dz=dz, dc=dc) for dz in steps for dc in range(nc) if (dz, dc) != (0, 0)]
    if tp > 1:
        peers += [device(dy=d) for d in (1, -1, 2)] + [device(dx=d) for d in (1, -1, 2)]
    for peer in peers:
        pl.semaphore_signal(barrier, inc=1, device_id=peer, device_id_type=MESH)

    my_cols = pl.ds(pl.multiple_of((y * nx + x) * 128, 128), 128)
    loads = [
        pltpu.make_async_copy(src, dst, local_sems.at[i])
        for i, (src, dst) in enumerate(
            [
                (retain_hbm, retain),
                (least_hbm, least),
                (extra_hbm, extra),
                (entries_hbm, entries),
                (asker_hbm, asker),
                (emit_hbm, emit),
                (lane_gain_hbm, lane_gain),
                (ids_hbm, ids),
                (chance_hbm, chance),
                (duo_hbm, duo),
                (project_hbm, project),
                (skip_hbm.at[:, my_cols], skip),
                (row_gain_hbm, row_gain),
                (switch_hbm, switch),
                (raise_hbm, raised),
                (lower_hbm, lower),
            ]
        )
    ]
    for load in loads:
        load.start()
    for load in loads[:4]:
        load.wait()

    spots = lax.broadcasted_iota(jnp.int32, (half, half), 0)
    other = lax.broadcasted_iota(jnp.int32, (half, half), 1)
    causal = spots >= other
    causal_ones = jnp.where(causal, 1.0, 0.0).astype(F32)
    eye_half = spots == other

    def decays(b):
        mine = pl.ds(b * half, half)
        floor = least[...]
        share = floor + (1.0 - floor) * jax.nn.sigmoid(retain[mine, :].astype(F32))
        logs = jnp.log(share) + column_of(extra[:, b * half : (b + 1) * half], eye_half)
        total = jnp.dot(causal_ones, logs, precision=HIGH, preferred_element_type=F32)
        return total, 1.0 - share

    states, lasts, kept = [], [], []
    for b in range(2):
        total, keys = decays(b)
        last = total[half - 1 : half, :]
        ending = keys * jnp.exp(last - total)
        values = entries[b * half : (b + 1) * half, :].astype(F32)
        states.append(dims_of(values, ending, 0, 0, HIGH))
        lasts.append(last)
        kept.append((total, keys))
    own_decay = jnp.exp(lasts[0] + lasts[1])
    state_first[...] = states[0]
    state_own[...] = jnp.exp(lasts[1]) * states[0] + states[1]

    tail_row = lax.broadcasted_iota(jnp.int32, (16, 128), 0)

    def pack(ref, value, decay):
        top = decay.astype(BF)
        low = (decay - top.astype(F32)).astype(BF)
        ref[0:64, :] = value.astype(BF)
        tail = jnp.where(
            tail_row == 0, top.astype(F32), jnp.where(tail_row == 1, low.astype(F32), 0.0)
        )
        ref[64:80, :] = tail.astype(BF)

    def unpack(ref):
        tail = ref[64:80, :].astype(F32)
        return ref[0:64, :].astype(F32), tail[0:1, :] + tail[1:2, :]

    first_core = c == 0
    mine_half = jnp.where(first_core, state_own[0:64, :], state_own[64:128, :])
    theirs_half = jnp.where(first_core, state_own[64:128, :], state_own[0:64, :])
    pack(half_out, theirs_half, own_decay)

    pl.semaphore_wait(barrier, len(peers))

    for load in loads[4:10]:
        load.wait()
    n_half = wire.slots(1)
    n_near = wire.slots(3)
    n_far = wire.slots(3)
    n_back = wire.slots(1)
    wire.send(half_out, half_in, n_half, partner)

    def score_block(b):
        total, keys = kept[b]
        mine = pl.ds(b * half, half)
        middle = total[half // 2 - 1 : half // 2, :]
        asked = jax.nn.silu(asker[mine, :].astype(F32))
        query_hat[mine, :] = asked * jnp.exp(total)
        scores = dims_of(
            asked * jnp.exp(total - middle), keys * jnp.exp(middle - total), 1, 1, HIGH
        )
        scores = jnp.where(causal, scores, 0.0)
        values = entries[mine, :].astype(F32)
        inside[mine, :] = jnp.dot(scores, values, precision=HIGH, preferred_element_type=F32)
        gates[mine, :] = lane_gain[...] * jax.nn.silu(emit[mine, :].astype(F32))

    wire.arrived(half_in, n_half, partner)
    theirs, their_decay = unpack(half_in)
    s0 = jnp.where(first_core, mine_half, theirs)
    s1 = jnp.where(first_core, theirs, mine_half)
    d0 = jnp.where(first_core, own_decay, their_decay)
    d1 = jnp.where(first_core, their_decay, own_decay)
    group, place = z // 4, lax.rem(z, 4)
    pack(near.at[place], d1 * s0 + s1, d0 * d1)

    def in_group(j):
        return (group * 4 + lax.rem(place + j, 4), c, y, x)

    for j in (1, 2, 3):
        wire.send(near.at[place], near.at[place], n_near + j - 1, in_group(j))

    score_block(0)
    score_block(1)

    for j in (1, 2, 3):
        sender = lax.rem(place + 4 - j, 4)
        wire.arrived(near.at[sender], n_near + j - 1, in_group(4 - j))
    before = jnp.zeros((64, 128), F32)
    before_decay = jnp.ones((1, 128), F32)
    total_state, total_decay = before, before_decay
    for j in range(4):
        value, decay = unpack(near.at[j])
        total_state = decay * total_state + value
        total_decay = decay * total_decay
        earlier = j < place
        before = jnp.where(earlier, decay * before + value, before)
        before_decay = jnp.where(earlier, decay * before_decay, before_decay)
    pack(far.at[group], total_state, total_decay)

    def to_group(j):
        return (lax.rem(z + 4 * j, nz), c, y, x)

    for j in range(1, groups):

        @pl.when(group + j < groups)
        def _():
            wire.copy(far.at[group], far.at[group], n_far + j - 1, to_group(j)).start()

    tok_row = lax.broadcasted_iota(jnp.int32, (tokens, tokens), 0)
    tok_col = lax.broadcasted_iota(jnp.int32, (tokens, tokens), 1)
    eye = tok_row == tok_col
    earlier_ones = jnp.where(tok_row < tok_col, 1.0, 0.0).astype(BF)
    experts = nz * nc
    expert_at = lax.broadcasted_iota(jnp.int32, (experts, tokens), 0)
    named = [jnp.where(expert_at == ids[j : j + 1, :], 1.0, 0.0).astype(F32) for j in range(2)]
    counts = jnp.dot(
        (named[0] + named[1]).astype(BF), earlier_ones, preferred_element_type=F32
    )
    slot_rows = [
        ids[j : j + 1, :].astype(F32) * cap + jnp.sum(counts * named[j], axis=0, keepdims=True)
        for j in range(2)
    ]
    slot_at = lax.broadcasted_iota(jnp.int32, (experts * cap, tokens), 0).astype(F32)
    select_in[...] = jnp.where(
        slot_at == slot_rows[0], 1.0, jnp.where(slot_at == slot_rows[1], 1.0, 0.0)
    ).astype(BF)
    slot_along = lax.broadcasted_iota(jnp.int32, (tokens, experts * cap), 1).astype(F32)
    spread = duo[0:1, :] - duo[1:2, :]
    for j in range(2):
        select_out[j] = jnp.where(
            slot_along == column_of(slot_rows[j], eye), 1.0, 0.0
        ).astype(BF)
        weight = chance[...] * jax.nn.sigmoid(spread if j == 0 else -spread)
        route[j] = jnp.broadcast_to(column_of(weight, eye), (tokens, 128))

    prefix[...] = jnp.zeros((64, 128), F32)
    for j in range(groups - 1):

        @pl.when(j < group)
        def _():
            sender = j
            number = n_far + group - 1 - j
            wire.arrived(far.at[sender], number, to_group(0))
            value, decay = unpack(far.at[sender])
            prefix[...] = decay * prefix[...] + value

    start = before_decay * prefix[...] + before
    after_first = d0 * start + s0
    back_out[...] = jnp.where(first_core, after_first, start).astype(BF)
    wire.send(back_out, back_in, n_back, partner)
    own_start = jnp.where(first_core, start, after_first)
    wire.arrived(back_in, n_back, partner)
    got = back_in[...].astype(F32)
    carried = jnp.concatenate(
        [jnp.where(first_core, own_start, got), jnp.where(first_core, got, own_start)], axis=0
    )
    for j in range(1, groups):

        @pl.when(group + j < groups)
        def _():
            wire.copy(far.at[group], far.at[group], n_far + j - 1, to_group(j)).wait_send()

    second = jnp.exp(lasts[0]) * carried + state_first[...]
    loads[10].wait()
    for b, state in enumerate((carried, second)):
        mine = pl.ds(b * half, half)
        readout = inside[mine, :] + dims_of(query_hat[mine, :], state, 1, 1, HIGH)
        mean = jnp.mean(readout * readout, axis=1, keepdims=True)
        mixed = (readout * lax.rsqrt(mean + EPS) * gates[mine, :]).astype(BF)
        for t in range(0, tp, 2):
            wide = jnp.dot(
                mixed, project[:, t * 128 : (t + 2) * 128], preferred_element_type=F32
            )
            for u in range(t, min(t + 2, tp)):
                mix_part[u // nx, u % nx, b] = (
                    wide[:, (u - t) * 128 : (u - t + 1) * 128]
                    .reshape(2, half // 2, 128)
                    .astype(BF)
                )

    ways = (2, 1, -1)

    class Reduce:
        def __init__(self, source, lo, n, direct, one, two, total, three):
            self.source, self.lo, self.n, self.direct = source, lo, n, direct
            self.one, self.two, self.total, self.three = one, two, total, three
            self.each = 6 if direct else 7
            self.first = wire.slots(2 * self.each)

        def at(self, k, f, g):
            rest = (k, pl.ds(self.lo, self.n))
            return self.source.at[(f, g) + rest] if k == 0 else self.source.at[(g, f) + rest]

        def axes(self, k):
            f, g = (y, x) if k == 0 else (x, y)
            name_f, name_g = ("dy", "dx") if k == 0 else ("dx", "dy")
            return f, g, (lambda d: device(**{name_f: d})), (lambda d: device(**{name_g: d}))

        def number(self, k, i):
            return self.first + k * self.each + i

        def step_one(self):
            for k in range(2):
                f, g, to_f, to_g = self.axes(k)
                if self.direct:
                    for way, delta in enumerate(ways):
                        wire.send(
                            self.at(k, lax.rem(f + delta + 4, 4), pl.ds(0, 4)),
                            self.one.at[k, way],
                            self.number(k, way),
                            to_f(delta),
                        )
                    continue
                across = lax.rem(f + 2, 4)
                for way, delta in ((0, 1), (1, -1)):
                    wire.send(
                        self.at(k, across, pl.ds(2 * way, 2)),
                        self.one.at[k, way],
                        self.number(k, way),
                        to_f(delta),
                    )

        def step_two(self):
            for k in range(2):
                f, g, to_f, to_g = self.axes(k)
                for way, delta in ((0, 1), (1, -1)):
                    wire.arrived(self.one.at[k, way], self.number(k, way), to_f(-delta))
                    mine = self.at(k, lax.rem(f + delta + 4, 4), pl.ds(2 * way, 2))
                    mine[...] = (mine[...].astype(F32) + self.one[k, way].astype(F32)).astype(BF)
            for k in range(2):
                f, g, to_f, to_g = self.axes(k)
                for way, delta in ((0, 1), (1, -1)):
                    wire.send(
                        self.at(k, lax.rem(f + delta + 4, 4), pl.ds(0, 4)),
                        self.two.at[k, way],
                        self.number(k, 2 + way),
                        to_f(delta),
                    )

        def inner(self):
            if self.direct:
                return [(self.one, way, delta, way) for way, delta in enumerate(ways)]
            return [(self.two, way, delta, 2 + way) for way, delta in ((0, 1), (1, -1))]

        def step_three(self):
            for k in range(2):
                f, g, to_f, to_g = self.axes(k)
                value = self.at(k, f, pl.ds(0, 4))[...].astype(F32)
                for buf, way, delta, i in self.inner():
                    wire.arrived(buf.at[k, way], self.number(k, i), to_f(-delta))
                    value = value + buf[k, way].astype(F32)
                self.total[k] = value.astype(BF)
            for k in range(2):
                f, g, to_f, to_g = self.axes(k)
                for way, delta in enumerate(ways):
                    wire.send(
                        self.total.at[k, lax.rem(g + delta + 4, 4)],
                        self.three.at[k, way],
                        self.number(k, self.each - 3 + way),
                        to_g(delta),
                    )

        def result(self, k):
            f, g, to_f, to_g = self.axes(k)
            value = self.at(k, f, g)[...].astype(F32)
            for buf, way, delta, i in self.inner():
                value = value + buf[k, way, g].astype(F32)
            for way, delta in enumerate(ways):
                wire.arrived(
                    self.three.at[k, way], self.number(k, self.each - 3 + way), to_g(-delta)
                )
                value = value + self.three[k, way].astype(F32)
            return value

    loads[11].wait()
    if tp > 1:
        mix = Reduce(mix_part, 0, 2, True, mix_one, None, mix_sum, mix_three)
        mix.step_one()
        mix.step_three()
        own_cols = [mix.result(k).reshape(half, 128) for k in range(2)]
    else:
        own_cols = [mix_part[0, 0, k].astype(F32).reshape(half, 128) for k in range(2)]
    for k in range(2):
        mine = pl.ds(k * half, half)
        skip[mine, :] = (skip[mine, :].astype(F32) + own_cols[k]).astype(BF)

    tiles = cap // TILE
    slots[...] = (
        jnp.dot(select_in[...], skip[...], preferred_element_type=F32)
        .reshape(experts, tiles, TILE, 128)
        .astype(BF)
    )
    rows[y, x, 0, 0] = slots[me_sp]
    n_out = wire.slots(nz * nc)
    for i, dz in enumerate(steps):
        for dc in range(nc):
            if (dz, dc) == (0, 0):
                continue
            there = device(dz=dz, dc=dc)
            wire.send(
                slots.at[there[0] * nc + there[1]],
                rows.at[y, x, dc, i],
                n_out + i * nc + dc,
                there,
            )

    class Chunk:
        def __init__(self, number):
            self.lo = number * CHUNK
            self.number = number
            if tp > 1:
                self.first = wire.slots(14)
                self.red = Reduce(
                    part,
                    self.lo,
                    CHUNK,
                    False,
                    *(b.at[number] for b in (red_one, red_two, red_sum, red_three)),
                )

        def at(self, k, p, s, lo=0, n=CHUNK):
            rest = (k, pl.ds(self.lo + lo, n))
            return rows.at[(s, p) + rest] if k == 0 else rows.at[(p, s) + rest]

        def axes(self, k):
            p, s = (x, y) if k == 0 else (y, x)
            name_p, name_s = ("dx", "dy") if k == 0 else ("dy", "dx")
            return p, s, (lambda d: device(**{name_p: d})), (lambda d: device(**{name_s: d}))

        def sem(self, k, i):
            return self.first + k * 7 + i

        def gather_one(self):
            for i in range(self.lo, self.lo + CHUNK):
                for dc in range(nc):
                    if (steps[i], dc) != (0, 0):
                        wire.arrived(
                            rows.at[y, x, dc, i], n_out + i * nc + dc, device(dz=-steps[i], dc=dc)
                        )
            if tp == 1:
                return
            for k in range(2):
                p, s, to_p, to_s = self.axes(k)
                mine = self.at(k, p, s)
                for way, delta in enumerate(ways):
                    wire.send(mine, mine, self.sem(k, way), to_p(delta))

        def gather_two(self):
            for k in range(2 if tp > 1 else 0):
                p, s, to_p, to_s = self.axes(k)
                for way, delta in enumerate(ways):
                    came = lax.rem(p - delta + 4, 4)
                    wire.arrived(self.at(k, came, s), self.sem(k, way), to_p(-delta))
                mine = self.at(k, pl.ds(0, 4), s)
                for way, delta in ((0, 1), (1, -1)):
                    wire.send(mine, mine, self.sem(k, 3 + way), to_s(delta))

        def gather_three(self):
            for k in range(2 if tp > 1 else 0):
                p, s, to_p, to_s = self.axes(k)
                for way, delta in ((0, 1), (1, -1)):
                    came = lax.rem(s - delta + 4, 4)
                    wire.arrived(self.at(k, pl.ds(0, 4), came), self.sem(k, 3 + way), to_s(-delta))
                    onward = self.at(k, pl.ds(2 * way, 2), came)
                    wire.send(onward, onward, self.sem(k, 5 + way), to_s(delta))

        def experts(self):
            for k in range(2 if tp > 1 else 0):
                p, s, to_p, to_s = self.axes(k)
                across = lax.rem(s + 2, 4)
                for way, delta in ((0, 1), (1, -1)):
                    wire.arrived(
                        self.at(k, pl.ds(2 * way, 2), across), self.sem(k, 5 + way), to_s(-delta)
                    )
            span = pl.ds(self.lo, CHUNK)
            count = nc * CHUNK * cap
            squares = jnp.zeros((count, 128), F32)
            for t in range(tp):
                wide = rows[t // nx, t % nx, :, span].astype(F32).reshape(count, 128)
                squares = squares + wide * wide
            scale = lax.rsqrt(jnp.sum(squares, axis=1, keepdims=True) / (tp * 128) + EPS)
            for t in range(tp):
                wide = rows[t // nx, t % nx, :, span].astype(F32).reshape(count, 128)
                cols = slice(t * 128, (t + 1) * 128)
                normed[:, cols] = (wide * scale * row_gain[:, cols]).astype(BF)
            gate_acts = jnp.dot(normed[...], switch[...], preferred_element_type=F32)
            up_acts = jnp.dot(normed[...], raised[...], preferred_element_type=F32)
            hidden = (jax.nn.silu(gate_acts) * up_acts).astype(BF)
            for t in range(0, tp, 2):
                wide = jnp.dot(
                    hidden, lower[:, t * 128 : (t + 2) * 128], preferred_element_type=F32
                )
                for u in range(t, min(t + 2, tp)):
                    part[u // nx, u % nx, :, span] = (
                        wide[:, (u - t) * 128 : (u - t + 1) * 128]
                        .reshape(nc, CHUNK, tiles, TILE, 128)
                        .astype(BF)
                    )
            if tp > 1:
                self.red.step_one()

        def sum_two(self):
            if tp > 1:
                self.red.step_two()

        def sum_three(self):
            if tp > 1:
                self.red.step_three()

        def give_back(self):
            for k in range(2):
                if tp > 1:
                    done = self.red.result(k).astype(BF)
                else:
                    done = part[0, 0, k, pl.ds(self.lo, CHUNK)]
                finished[k, pl.ds(self.lo, CHUNK)] = done
            for i in range(self.lo, self.lo + CHUNK):
                for dc in range(nc):
                    if (steps[i], dc) == (0, 0):
                        returned[me_sp] = finished[0, 0]
                        continue
                    wire.send(
                        finished.at[dc, i],
                        returned.at[me_sp],
                        n_back_rows + i * nc + dc,
                        device(dz=-steps[i], dc=dc),
                    )

    n_back_rows = wire.slots(nz * nc)
    work = [Chunk(n) for n in range(chunks)]
    for load in loads[12:]:
        load.wait()
    order = (
        "gather_one",
        "gather_two",
        "gather_three",
        "experts",
        "sum_two",
        "sum_three",
        "give_back",
    )
    tasks = sorted((2 * j + n, n, j) for n in range(chunks) for j in range(len(order)))
    for _, n, j in tasks:
        getattr(work[n], order[j])()

    for i, dz in enumerate(steps):
        for dc in range(nc):
            if (dz, dc) == (0, 0):
                continue
            there = device(dz=dz, dc=dc)
            wire.arrived(
                returned.at[there[0] * nc + there[1]], n_back_rows + i * nc + dc, there
            )
    got_rows = returned[...].astype(F32).reshape(experts * cap, 128).astype(BF)
    result = skip[...].astype(F32)
    for j in range(2):
        picked = jnp.dot(select_out[j], got_rows, preferred_element_type=F32)
        result = result + route[j] * picked
    out[...] = result.astype(BF)
    for copy in wire.started:
        copy.wait_send()


def layer(
    sizes,
    skip_path_vectors,
    asker_raw_scores,
    retain_raw_scores,
    memory_write_entries,
    emit_switch_scores,
    retain_minimum_share,
    extra_shrink_rate,
    lane_rescale_factor,
    emit_projection_array,
    specialist_rescale_factor,
    specialist_switch_proj,
    specialist_raise_proj,
    specialist_lower_proj,
    specialist_choice_ids,
    cluster_chance,
    specialist_duo_scores,
):
    nz, nc, ny, nx, tokens, cap = sizes
    tp = ny * nx
    width = tp * 128
    hidden = specialist_switch_proj.shape[2]
    half, experts, chunks, tiles = tokens // 2, nz * nc, nz // CHUNK, cap // TILE
    block = (tiles, TILE, 128)
    vmem, anywhere = (
        pl.BlockSpec(memory_space=pltpu.VMEM),
        pl.BlockSpec(memory_space=pl.ANY),
    )
    count = semaphore_count(nz, nc, tp)
    scratch = [
        pltpu.VMEM((tokens, 128), BF),
        pltpu.VMEM((tokens, 128), BF),
        pltpu.VMEM((tokens, 128), BF),
        pltpu.VMEM((tokens, 128), BF),
        pltpu.VMEM((1, 128), F32),
        pltpu.VMEM((1, tokens), F32),
        pltpu.VMEM((1, 128), F32),
        pltpu.VMEM((1, width), F32),
        pltpu.VMEM((2, tokens), jnp.int32),
        pltpu.VMEM((1, tokens), F32),
        pltpu.VMEM((2, tokens), F32),
        pltpu.VMEM((tokens, 128), BF),
        pltpu.VMEM((128, width), BF),
        pltpu.VMEM((width, hidden), BF),
        pltpu.VMEM((width, hidden), BF),
        pltpu.VMEM((hidden, width), BF),
        pltpu.VMEM((128, 128), F32),
        pltpu.VMEM((128, 128), F32),
        pltpu.VMEM((80, 128), BF),
        pltpu.VMEM((80, 128), BF),
        pltpu.VMEM((4, 80, 128), BF),
        pltpu.VMEM((nz // 4, 80, 128), BF),
        pltpu.VMEM((64, 128), BF),
        pltpu.VMEM((64, 128), BF),
        pltpu.VMEM((64, 128), F32),
        pltpu.VMEM((tokens, 128), F32),
        pltpu.VMEM((tokens, 128), F32),
        pltpu.VMEM((tokens, 128), F32),
        pltpu.VMEM((experts * cap, tokens), BF),
        pltpu.VMEM((2, tokens, experts * cap), BF),
        pltpu.VMEM((2, tokens, 128), F32),
        pltpu.VMEM((ny, nx, 2, 2, half // 2, 128), BF),
        pltpu.VMEM((2, 3, 4, 2, half // 2, 128), BF),
        pltpu.VMEM((2, 4, 2, half // 2, 128), BF),
        pltpu.VMEM((2, 3, 2, half // 2, 128), BF),
        pltpu.VMEM((experts, *block), BF),
        pltpu.VMEM((ny, nx, nc, nz, *block), BF),
        pltpu.VMEM((nc * CHUNK * cap, width), BF),
        pltpu.VMEM((ny, nx, nc, nz, *block), BF),
        pltpu.VMEM((chunks, 2, 2, 2, CHUNK, *block), BF),
        pltpu.VMEM((chunks, 2, 2, 4, CHUNK, *block), BF),
        pltpu.VMEM((chunks, 2, 4, CHUNK, *block), BF),
        pltpu.VMEM((chunks, 2, 3, CHUNK, *block), BF),
        pltpu.VMEM((nc, nz, *block), BF),
        pltpu.VMEM((experts, *block), BF),
        pltpu.SemaphoreType.DMA((16,)),
        pltpu.SemaphoreType.DMA((count,)),
        pltpu.SemaphoreType.DMA((count,)),
    ]
    return pl.pallas_call(
        functools.partial(kernel, sizes),
        out_shape=jax.ShapeDtypeStruct((tokens, 128), BF),
        in_specs=[anywhere] * 16,
        out_specs=vmem,
        scratch_shapes=scratch,
        compiler_params=pltpu.CompilerParams(collective_id=0, has_side_effects=True),
    )(
        asker_raw_scores,
        retain_raw_scores,
        memory_write_entries,
        emit_switch_scores,
        retain_minimum_share.reshape(1, 128),
        extra_shrink_rate,
        lane_rescale_factor.reshape(1, 128),
        specialist_rescale_factor.reshape(1, width),
        specialist_choice_ids.T,
        cluster_chance.reshape(1, tokens),
        specialist_duo_scores.T,
        skip_path_vectors,
        emit_projection_array,
        specialist_switch_proj[0],
        specialist_raise_proj[0],
        specialist_lower_proj[0],
    )


def solution(mesh, shape=(16, 2, 4, 4), tokens=256, cap=24):
    finer = Mesh(mesh.devices.reshape(shape), AXES)
    in_specs = (
        P(SP, None),
        P(SP, TP),
        P(SP, TP),
        P(SP, TP),
        P(SP, TP),
        P(TP),
        P(TP, SP),
        P(),
        P(TP, None),
        P(),
        P(SP, None, TP),
        P(SP, None, TP),
        P(SP, TP, None),
        P(SP, None),
        P(SP),
        P(SP, None),
    )
    return jax.shard_map(
        functools.partial(layer, (*shape, tokens, cap)),
        mesh=finer,
        in_specs=in_specs,
        out_specs=P(SP, TP),
        check_vma=False,
    )
```

```python
import functools

import jax
import jax.numpy as jnp
from jax import lax
from jax.experimental import pallas as pl
from jax.experimental.pallas import tpu as pltpu
from jax.sharding import Mesh
from jax.sharding import PartitionSpec as P

AXES = ("z", "c", "y", "x")
SP = ("z", "c")
TP = ("y", "x")
EPS = 1e-06
BF = jnp.bfloat16
F32 = jnp.float32
HIGH = lax.Precision.HIGHEST
MESH = pl.DeviceIdType.MESH
TILE = 8
CHUNK = 4


def dims_of(a, b, left, right, precision=None):
    return lax.dot_general(
        a, b, (((left,), (right,)), ((), ())), precision=precision, preferred_element_type=F32
    )


def z_steps(count):
    steps = [0]
    for far in range(1, count // 2 + 1):
        steps += [far, -far]
    return steps[:count]


def column_of(row, eye):
    return jnp.sum(jnp.where(eye, row, 0.0), axis=1, keepdims=True)


class Wire:
    def __init__(self, sends, recvs):
        self.sends, self.recvs, self.used, self.started = sends, recvs, 0, []

    def slots(self, count):
        first = self.used
        self.used += count
        return first

    def copy(self, src, dst, number, device):
        return pltpu.make_async_remote_copy(
            src_ref=src,
            dst_ref=dst,
            send_sem=self.sends.at[number],
            recv_sem=self.recvs.at[number],
            device_id=device,
            device_id_type=MESH,
        )

    def send(self, src, dst, number, device):
        copy = self.copy(src, dst, number, device)
        copy.start()
        self.started.append(copy)

    def arrived(self, dst, number, device):
        self.copy(dst, dst, number, device).wait_recv()


def semaphore_count(nz, nc, tp):
    return 1 + 3 + 3 + 1 + 6 + 12 + 2 * nz + 26 * (nz // CHUNK)


def kernel(
    sizes,
    asker_hbm,
    retain_hbm,
    entries_hbm,
    emit_hbm,
    least_hbm,
    extra_hbm,
    lane_gain_hbm,
    row_gain_hbm,
    ids_hbm,
    chance_hbm,
    duo_hbm,
    skip_hbm,
    project_hbm,
    switch_hbm,
    raise_hbm,
    lower_hbm,
    out,
    asker,
    retain,
    entries,
    emit,
    least,
    extra,
    lane_gain,
    row_gain,
    ids,
    chance,
    duo,
    skip,
    project,
    switch,
    raised,
    lower,
    state_own,
    state_first,
    half_out,
    half_in,
    near,
    far,
    back_out,
    back_in,
    prefix,
    query_hat,
    inside,
    gates,
    select_in,
    select_out,
    route,
    mix_part,
    mix_one,
    mix_sum,
    mix_three,
    slots,
    bands,
    rows,
    normed,
    part,
    other_part,
    summed,
    red_one,
    red_a,
    red_b,
    last_a,
    last_b,
    finished,
    returned,
    local_sems,
    sends,
    recvs,
):
    nz, nc, ny, nx, tokens, cap = sizes
    tp = ny * nx
    groups = nz // 4
    half = tokens // 2
    z, c, y, x = (lax.axis_index(a) for a in AXES)
    me_sp = z * nc + c
    wire = Wire(sends, recvs)
    steps = z_steps(nz)
    chunks = nz // CHUNK
    mine_expert = lax.rem(x, 2)
    keeps = c == mine_expert

    def device(dz=0, dc=0, dy=0, dx=0):
        return (
            lax.rem(z + (dz + nz), nz),
            lax.rem(c + dc, nc),
            lax.rem(y + (dy + ny), ny),
            lax.rem(x + (dx + nx), nx),
        )

    partner = device(dc=1)
    barrier = pltpu.get_barrier_semaphore()
    peers = [partner] + [device(dz=dz) for dz in steps[1:]]
    peers += [device(dy=d) for d in (1, -1, 2)] + [device(dx=d) for d in (1, -1, 2)]
    peers += [device(dx=d, dc=1) for d in (1, -1)]
    for peer in peers:
        pl.semaphore_signal(barrier, inc=1, device_id=peer, device_id_type=MESH)

    my_cols = pl.ds(pl.multiple_of((y * nx + x) * 128, 128), 128)
    loads = [
        pltpu.make_async_copy(src, dst, local_sems.at[i])
        for i, (src, dst) in enumerate(
            [
                (retain_hbm, retain),
                (least_hbm, least),
                (extra_hbm, extra),
                (entries_hbm, entries),
                (asker_hbm, asker),
                (emit_hbm, emit),
                (lane_gain_hbm, lane_gain),
                (ids_hbm, ids),
                (chance_hbm, chance),
                (duo_hbm, duo),
                (project_hbm, project),
                (skip_hbm.at[:, my_cols], skip),
                (row_gain_hbm, row_gain),
            ]
        )
    ]
    for load in loads:
        load.start()
    own_weights = [
        pltpu.make_async_copy(src, dst, local_sems.at[13 + i])
        for i, (src, dst) in enumerate(
            [(switch_hbm, switch), (raise_hbm, raised), (lower_hbm, lower)]
        )
    ]

    @pl.when(keeps)
    def _():
        for load in own_weights:
            load.start()

    for load in loads[:4]:
        load.wait()

    spots = lax.broadcasted_iota(jnp.int32, (half, half), 0)
    other = lax.broadcasted_iota(jnp.int32, (half, half), 1)
    causal = spots >= other
    causal_ones = jnp.where(causal, 1.0, 0.0).astype(F32)
    eye_half = spots == other

    def decays(b):
        mine = pl.ds(b * half, half)
        floor = least[...]
        share = floor + (1.0 - floor) * jax.nn.sigmoid(retain[mine, :].astype(F32))
        logs = jnp.log(share) + column_of(extra[:, b * half : (b + 1) * half], eye_half)
        total = jnp.dot(causal_ones, logs, precision=HIGH, preferred_element_type=F32)
        return total, 1.0 - share

    states, lasts, kept = [], [], []
    for b in range(2):
        total, keys = decays(b)
        last = total[half - 1 : half, :]
        ending = keys * jnp.exp(last - total)
        values = entries[b * half : (b + 1) * half, :].astype(F32)
        states.append(dims_of(values, ending, 0, 0, HIGH))
        lasts.append(last)
        kept.append((total, keys))
    own_decay = jnp.exp(lasts[0] + lasts[1])
    state_first[...] = states[0]
    state_own[...] = jnp.exp(lasts[1]) * states[0] + states[1]

    tail_row = lax.broadcasted_iota(jnp.int32, (16, 128), 0)

    def pack(ref, value, decay):
        top = decay.astype(BF)
        low = (decay - top.astype(F32)).astype(BF)
        ref[0:64, :] = value.astype(BF)
        tail = jnp.where(
            tail_row == 0, top.astype(F32), jnp.where(tail_row == 1, low.astype(F32), 0.0)
        )
        ref[64:80, :] = tail.astype(BF)

    def unpack(ref):
        tail = ref[64:80, :].astype(F32)
        return ref[0:64, :].astype(F32), tail[0:1, :] + tail[1:2, :]

    first_core = c == 0
    mine_half = jnp.where(first_core, state_own[0:64, :], state_own[64:128, :])
    theirs_half = jnp.where(first_core, state_own[64:128, :], state_own[0:64, :])
    pack(half_out, theirs_half, own_decay)

    pl.semaphore_wait(barrier, len(peers))

    for load in loads[4:10]:
        load.wait()
    n_half = wire.slots(1)
    n_near = wire.slots(3)
    n_far = wire.slots(3)
    n_back = wire.slots(1)
    wire.send(half_out, half_in, n_half, partner)

    n_weights = wire.slots(6)
    part_width = switch.shape[1] // 2

    def moved(way, delta):
        cut = slice(way * part_width, (way + 1) * part_width)
        refs = [
            (switch_hbm.at[:, cut], switch.at[:, cut]),
            (raise_hbm.at[:, cut], raised.at[:, cut]),
            (lower_hbm.at[cut, :], lower.at[cut, :]),
        ]
        there = device(dx=delta, dc=1)
        return [
            wire.copy(src, dst, n_weights + 3 * way + i, there) for i, (src, dst) in enumerate(refs)
        ]

    moves = moved(0, 1) + moved(1, -1)

    @pl.when(jnp.logical_not(keeps))
    def _():
        for copy in moves:
            copy.start()


    def score_block(b):
        total, keys = kept[b]
        mine = pl.ds(b * half, half)
        middle = total[half // 2 - 1 : half // 2, :]
        asked = jax.nn.silu(asker[mine, :].astype(F32))
        query_hat[mine, :] = asked * jnp.exp(total)
        scores = dims_of(
            asked * jnp.exp(total - middle), keys * jnp.exp(middle - total), 1, 1, HIGH
        )
        scores = jnp.where(causal, scores, 0.0)
        values = entries[mine, :].astype(F32)
        inside[mine, :] = jnp.dot(scores, values, precision=HIGH, preferred_element_type=F32)
        gates[mine, :] = lane_gain[...] * jax.nn.silu(emit[mine, :].astype(F32))

    wire.arrived(half_in, n_half, partner)
    theirs, their_decay = unpack(half_in)
    s0 = jnp.where(first_core, mine_half, theirs)
    s1 = jnp.where(first_core, theirs, mine_half)
    d0 = jnp.where(first_core, own_decay, their_decay)
    d1 = jnp.where(first_core, their_decay, own_decay)
    group, place = z // 4, lax.rem(z, 4)
    pack(near.at[place], d1 * s0 + s1, d0 * d1)

    def in_group(j):
        return (group * 4 + lax.rem(place + j, 4), c, y, x)

    for j in (1, 2, 3):
        wire.send(near.at[place], near.at[place], n_near + j - 1, in_group(j))

    score_block(0)
    score_block(1)

    for j in (1, 2, 3):
        sender = lax.rem(place + 4 - j, 4)
        wire.arrived(near.at[sender], n_near + j - 1, in_group(4 - j))
    before = jnp.zeros((64, 128), F32)
    before_decay = jnp.ones((1, 128), F32)
    total_state, total_decay = before, before_decay
    for j in range(4):
        value, decay = unpack(near.at[j])
        total_state = decay * total_state + value
        total_decay = decay * total_decay
        earlier = j < place
        before = jnp.where(earlier, decay * before + value, before)
        before_decay = jnp.where(earlier, decay * before_decay, before_decay)
    pack(far.at[group], total_state, total_decay)

    def to_group(j):
        return (lax.rem(z + 4 * j, nz), c, y, x)

    for j in range(1, groups):

        @pl.when(group + j < groups)
        def _():
            wire.copy(far.at[group], far.at[group], n_far + j - 1, to_group(j)).start()

    tok_row = lax.broadcasted_iota(jnp.int32, (tokens, tokens), 0)
    tok_col = lax.broadcasted_iota(jnp.int32, (tokens, tokens), 1)
    eye = tok_row == tok_col
    earlier_ones = jnp.where(tok_row < tok_col, 1.0, 0.0).astype(BF)
    experts = nz * nc
    expert_at = lax.broadcasted_iota(jnp.int32, (experts, tokens), 0)
    named = [jnp.where(expert_at == ids[j : j + 1, :], 1.0, 0.0).astype(F32) for j in range(2)]
    counts = jnp.dot(
        (named[0] + named[1]).astype(BF), earlier_ones, preferred_element_type=F32
    )
    slot_rows = [
        ids[j : j + 1, :].astype(F32) * cap + jnp.sum(counts * named[j], axis=0, keepdims=True)
        for j in range(2)
    ]
    slot_at = lax.broadcasted_iota(jnp.int32, (experts * cap, tokens), 0).astype(F32)
    select_in[...] = jnp.where(
        slot_at == slot_rows[0], 1.0, jnp.where(slot_at == slot_rows[1], 1.0, 0.0)
    ).astype(BF)
    slot_along = lax.broadcasted_iota(jnp.int32, (tokens, experts * cap), 1).astype(F32)
    spread = duo[0:1, :] - duo[1:2, :]
    for j in range(2):
        select_out[j] = jnp.where(
            slot_along == column_of(slot_rows[j], eye), 1.0, 0.0
        ).astype(BF)
        weight = chance[...] * jax.nn.sigmoid(spread if j == 0 else -spread)
        route[j] = jnp.broadcast_to(column_of(weight, eye), (tokens, 128))

    prefix[...] = jnp.zeros((64, 128), F32)
    for j in range(groups - 1):

        @pl.when(j < group)
        def _():
            sender = j
            number = n_far + group - 1 - j
            wire.arrived(far.at[sender], number, to_group(0))
            value, decay = unpack(far.at[sender])
            prefix[...] = decay * prefix[...] + value

    start = before_decay * prefix[...] + before
    after_first = d0 * start + s0
    back_out[...] = jnp.where(first_core, after_first, start).astype(BF)
    wire.send(back_out, back_in, n_back, partner)
    own_start = jnp.where(first_core, start, after_first)
    wire.arrived(back_in, n_back, partner)
    got = back_in[...].astype(F32)
    carried = jnp.concatenate(
        [jnp.where(first_core, own_start, got), jnp.where(first_core, got, own_start)], axis=0
    )
    for j in range(1, groups):

        @pl.when(group + j < groups)
        def _():
            wire.copy(far.at[group], far.at[group], n_far + j - 1, to_group(j)).wait_send()

    second = jnp.exp(lasts[0]) * carried + state_first[...]
    loads[10].wait()
    for b, state in enumerate((carried, second)):
        mine = pl.ds(b * half, half)
        readout = inside[mine, :] + dims_of(query_hat[mine, :], state, 1, 1, HIGH)
        mean = jnp.mean(readout * readout, axis=1, keepdims=True)
        mixed = (readout * lax.rsqrt(mean + EPS) * gates[mine, :]).astype(BF)
        for t in range(0, tp, 2):
            wide = jnp.dot(
                mixed, project[:, t * 128 : (t + 2) * 128], preferred_element_type=F32
            )
            for u in range(t, min(t + 2, tp)):
                mix_part[u // nx, u % nx, b] = (
                    wide[:, (u - t) * 128 : (u - t + 1) * 128]
                    .reshape(2, half // 2, 128)
                    .astype(BF)
                )

    ways = (2, 1, -1)

    class Reduce:
        def __init__(self, source, lo, n, one, total, three):
            self.source, self.one, self.total, self.three = source, one, total, three
            self.first = wire.slots(12)
            self.span = pl.ds(lo, n)
            self.every = pl.ds(0, 4)

        def at(self, k, f, g):
            rest = (k, self.span)
            return self.source.at[(f, g) + rest] if k == 0 else self.source.at[(g, f) + rest]

        def axes(self, k):
            f, g = (y, x) if k == 0 else (x, y)
            name_f, name_g = ("dy", "dx") if k == 0 else ("dx", "dy")
            return f, g, (lambda d: device(**{name_f: d})), (lambda d: device(**{name_g: d}))

        def step_one(self):
            for k in range(2):
                f, g, to_f, to_g = self.axes(k)
                for way, delta in enumerate(ways):
                    wire.send(
                        self.at(k, lax.rem(f + delta + 4, 4), self.every),
                        self.one.at[k, way, self.every, self.span],
                        self.first + k * 6 + way,
                        to_f(delta),
                    )

        def step_three(self):
            for k in range(2):
                f, g, to_f, to_g = self.axes(k)
                value = self.at(k, f, self.every)[...].astype(F32)
                for way, delta in enumerate(ways):
                    came = self.one.at[k, way, self.every, self.span]
                    wire.arrived(came, self.first + k * 6 + way, to_f(-delta))
                    value = value + came[...].astype(F32)
                self.total[k, self.every, self.span] = value.astype(BF)
            for k in range(2):
                f, g, to_f, to_g = self.axes(k)
                for way, delta in enumerate(ways):
                    wire.send(
                        self.total.at[k, lax.rem(g + delta + 4, 4), self.span],
                        self.three.at[k, way, self.span],
                        self.first + k * 6 + 3 + way,
                        to_g(delta),
                    )

        def result(self, k):
            f, g, to_f, to_g = self.axes(k)
            value = self.at(k, f, g)[...].astype(F32)
            for way, delta in enumerate(ways):
                value = value + self.one[k, way, g, self.span].astype(F32)
            for way, delta in enumerate(ways):
                came = self.three.at[k, way, self.span]
                wire.arrived(came, self.first + k * 6 + 3 + way, to_g(-delta))
                value = value + came[...].astype(F32)
            return value

    loads[11].wait()
    if tp > 1:
        mix = Reduce(mix_part, 0, 2, mix_one, mix_sum, mix_three)
        mix.step_one()
        mix.step_three()
        own_cols = [mix.result(k).reshape(half, 128) for k in range(2)]
    else:
        own_cols = [mix_part[0, 0, k].astype(F32).reshape(half, 128) for k in range(2)]
    for k in range(2):
        mine = pl.ds(k * half, half)
        skip[mine, :] = (skip[mine, :].astype(F32) + own_cols[k]).astype(BF)

    tiles = cap // TILE
    slots[...] = (
        jnp.dot(select_in[...], skip[...], preferred_element_type=F32)
        .reshape(experts, tiles, TILE, 128)
        .astype(BF)
    )
    n_out = wire.slots(nz)
    bands[y, :, 0] = slots[pl.ds(2 * z, 2)]
    for i, dz in enumerate(steps):
        if dz == 0:
            continue
        there = device(dz=dz)
        wire.send(
            slots.at[pl.ds(2 * there[0], 2)], bands.at[y, :, i], n_out + i, there
        )

    four = pl.ds(0, 4)

    class Chunk:
        def __init__(self, number):
            self.lo = number * CHUNK
            self.h = CHUNK // 2
            self.first = wire.slots(26)
            self.whole = pl.ds(self.lo, CHUNK)
            self.spans = [pl.ds(self.lo, self.h), pl.ds(self.lo + self.h, self.h)]

        def expert_for(self, delta):
            return mine_expert if delta == 2 else 1 - mine_expert

        def gather_one(self):
            for i in range(self.lo, self.lo + CHUNK):
                if steps[i] != 0:
                    wire.arrived(bands.at[y, :, i], n_out + i, device(dz=-steps[i]))
            a, b = self.spans
            for way, delta in enumerate(ways):
                wire.send(
                    bands.at[y, self.expert_for(delta), a],
                    rows.at[y, x, c, a],
                    self.first + way,
                    device(dx=delta),
                )
                both = bands.at[y, pl.ds(0, 2), b]
                wire.send(both, both, self.first + 3 + way, device(dy=delta))
            rows[y, x, c, a] = bands[y, mine_expert, a]

        def gather_two(self):
            a, b = self.spans
            for way, delta in enumerate(ways):
                came_x = lax.rem(x - delta + 4, 4)
                wire.arrived(rows.at[y, came_x, c, a], self.first + way, device(dx=-delta))
            for way, delta in enumerate(ways):
                quad = rows.at[y, four, c, a]
                wire.send(quad, quad, self.first + 6 + way, device(dy=delta))
            for way, delta in enumerate(ways):
                came_y = lax.rem(y - delta + 4, 4)
                wire.arrived(
                    bands.at[came_y, pl.ds(0, 2), b], self.first + 3 + way, device(dy=-delta)
                )
            for way, delta in enumerate(ways):
                wire.send(
                    bands.at[four, self.expert_for(delta), b],
                    rows.at[four, x, c, b],
                    self.first + 9 + way,
                    device(dx=delta),
                )
            rows[four, x, c, b] = bands[four, mine_expert, b]

        def gather_three(self):
            a, b = self.spans
            for way, delta in enumerate(ways):
                came_x, came_y = lax.rem(x - delta + 4, 4), lax.rem(y - delta + 4, 4)
                wire.arrived(
                    rows.at[came_y, four, c, a], self.first + 6 + way, device(dy=-delta)
                )
                wire.arrived(
                    rows.at[four, came_x, c, b], self.first + 9 + way, device(dx=-delta)
                )
            mine = rows.at[four, four, c, self.whole]
            wire.send(mine, mine, self.first + 12, partner)

        def experts(self):
            wire.arrived(rows.at[four, four, 1 - c, self.whole], self.first + 12, partner)
            count = nc * CHUNK * cap
            squares = jnp.zeros((count, 128), F32)
            for t in range(tp):
                wide = rows[t // nx, t % nx, :, self.whole].astype(F32).reshape(count, 128)
                squares = squares + wide * wide
            scale = lax.rsqrt(jnp.sum(squares, axis=1, keepdims=True) / (tp * 128) + EPS)
            for t in range(tp):
                wide = rows[t // nx, t % nx, :, self.whole].astype(F32).reshape(count, 128)
                cols = slice(t * 128, (t + 1) * 128)
                normed[:, cols] = (wide * scale * row_gain[:, cols]).astype(BF)
            gate_acts = jnp.dot(normed[...], switch[...], preferred_element_type=F32)
            up_acts = jnp.dot(normed[...], raised[...], preferred_element_type=F32)
            hidden = (jax.nn.silu(gate_acts) * up_acts).astype(BF)
            for t in range(0, tp, 2):
                wide = jnp.dot(
                    hidden, lower[:, t * 128 : (t + 2) * 128], preferred_element_type=F32
                )
                for u in range(t, t + 2):
                    part[u // nx, u % nx, :, self.whole] = (
                        wide[:, (u - t) * 128 : (u - t + 1) * 128]
                        .reshape(nc, CHUNK, tiles, TILE, 128)
                        .astype(BF)
                    )
            wire.send(
                part.at[four, four, 1 - c, self.whole],
                other_part.at[four, four, self.whole],
                self.first + 13,
                partner,
            )

        def sum_one(self):
            came = other_part.at[four, four, self.whole]
            wire.arrived(came, self.first + 13, partner)
            for t in range(tp):
                at = (t // nx, t % nx)
                summed[at[0], at[1], self.whole] = (
                    part[at[0], at[1], c, self.whole].astype(F32)
                    + other_part[at[0], at[1], self.whole].astype(F32)
                ).astype(BF)
            a, b = self.spans
            for way, delta in enumerate(ways):
                to_y, to_x = lax.rem(y + delta + 4, 4), lax.rem(x + delta + 4, 4)
                wire.send(
                    summed.at[to_y, four, a],
                    red_one.at[way, four, a],
                    self.first + 14 + way,
                    device(dy=delta),
                )
                wire.send(
                    summed.at[four, to_x, b],
                    red_one.at[way, four, b],
                    self.first + 17 + way,
                    device(dx=delta),
                )

        def first_sum(self, index):
            a = self.spans[0]
            value = summed[y, index, a].astype(F32)
            for way in range(3):
                value = value + red_one[way, index, a].astype(F32)
            return value

        def second_sums(self, index):
            b = self.spans[1]
            own = summed[index, x, b].astype(F32) + red_one[0, index, b].astype(F32)
            return own, red_one[1, index, b].astype(F32) + red_one[2, index, b].astype(F32)

        def sum_two(self):
            a, b = self.spans
            for way, delta in enumerate(ways):
                wire.arrived(
                    red_one.at[way, four, a], self.first + 14 + way, device(dy=-delta)
                )
                wire.arrived(
                    red_one.at[way, four, b], self.first + 17 + way, device(dx=-delta)
                )
            red_a[four, a] = self.first_sum(four).astype(BF)
            own, other = self.second_sums(four)
            red_b[four, mine_expert, b] = own.astype(BF)
            red_b[four, 1 - mine_expert, b] = other.astype(BF)
            for way, delta in enumerate(ways):
                to_y, to_x = lax.rem(y + delta + 4, 4), lax.rem(x + delta + 4, 4)
                wire.send(
                    red_a.at[to_x, a],
                    last_a.at[way, a],
                    self.first + 20 + way,
                    device(dx=delta),
                )
                wire.send(
                    red_b.at[to_y, pl.ds(0, 2), b],
                    last_b.at[way, pl.ds(0, 2), b],
                    self.first + 23 + way,
                    device(dy=delta),
                )

        def give_back(self):
            a, b = self.spans
            for way, delta in enumerate(ways):
                wire.arrived(last_a.at[way, a], self.first + 20 + way, device(dx=-delta))
                wire.arrived(
                    last_b.at[way, pl.ds(0, 2), b], self.first + 23 + way, device(dy=-delta)
                )
            finished[mine_expert, a] = (
                self.first_sum(x) + last_a[0, a].astype(F32)
            ).astype(BF)
            finished[1 - mine_expert, a] = (
                last_a[1, a].astype(F32) + last_a[2, a].astype(F32)
            ).astype(BF)
            own, other = self.second_sums(y)
            for expert, value in ((mine_expert, own), (1 - mine_expert, other)):
                for way in range(3):
                    value = value + last_b[way, expert, b].astype(F32)
                finished[expert, b] = value.astype(BF)
            for i in range(self.lo, self.lo + CHUNK):
                if steps[i] == 0:
                    returned[pl.ds(2 * z, 2)] = finished[:, i]
                    continue
                wire.send(
                    finished.at[pl.ds(0, 2), i],
                    returned.at[pl.ds(2 * z, 2)],
                    n_home + i,
                    device(dz=-steps[i]),
                )

    n_home = wire.slots(nz)
    work = [Chunk(n) for n in range(chunks)]
    loads[12].wait()

    @pl.when(keeps)
    def _():
        for load in own_weights:
            load.wait()

    @pl.when(jnp.logical_not(keeps))
    def _():
        for copy in moves:
            copy.wait_send()
            copy.wait_recv()

    order = (
        "gather_one",
        "gather_two",
        "gather_three",
        "experts",
        "sum_one",
        "sum_two",
        "give_back",
    )
    tasks = sorted((2 * j + n, n, j) for n in range(chunks) for j in range(len(order)))
    for _, n, j in tasks:
        getattr(work[n], order[j])()

    for i, dz in enumerate(steps):
        if dz != 0:
            there = device(dz=dz)
            wire.arrived(returned.at[pl.ds(2 * there[0], 2)], n_home + i, there)
    got_rows = returned[...].astype(F32).reshape(experts * cap, 128).astype(BF)
    result = skip[...].astype(F32)
    for j in range(2):
        picked = jnp.dot(select_out[j], got_rows, preferred_element_type=F32)
        result = result + route[j] * picked
    out[...] = result.astype(BF)
    for copy in wire.started:
        copy.wait_send()


def layer(
    sizes,
    skip_path_vectors,
    asker_raw_scores,
    retain_raw_scores,
    memory_write_entries,
    emit_switch_scores,
    retain_minimum_share,
    extra_shrink_rate,
    lane_rescale_factor,
    emit_projection_array,
    specialist_rescale_factor,
    specialist_switch_proj,
    specialist_raise_proj,
    specialist_lower_proj,
    specialist_choice_ids,
    cluster_chance,
    specialist_duo_scores,
):
    nz, nc, ny, nx, tokens, cap = sizes
    tp = ny * nx
    width = tp * 128
    hidden = specialist_switch_proj.shape[2]
    half, experts, tiles = tokens // 2, nz * nc, cap // TILE
    block = (tiles, TILE, 128)
    vmem, anywhere = (
        pl.BlockSpec(memory_space=pltpu.VMEM),
        pl.BlockSpec(memory_space=pl.ANY),
    )
    count = semaphore_count(nz, nc, tp)
    scratch = [
        pltpu.VMEM((tokens, 128), BF),
        pltpu.VMEM((tokens, 128), BF),
        pltpu.VMEM((tokens, 128), BF),
        pltpu.VMEM((tokens, 128), BF),
        pltpu.VMEM((1, 128), F32),
        pltpu.VMEM((1, tokens), F32),
        pltpu.VMEM((1, 128), F32),
        pltpu.VMEM((1, width), F32),
        pltpu.VMEM((2, tokens), jnp.int32),
        pltpu.VMEM((1, tokens), F32),
        pltpu.VMEM((2, tokens), F32),
        pltpu.VMEM((tokens, 128), BF),
        pltpu.VMEM((128, width), BF),
        pltpu.VMEM((width, hidden), BF),
        pltpu.VMEM((width, hidden), BF),
        pltpu.VMEM((hidden, width), BF),
        pltpu.VMEM((128, 128), F32),
        pltpu.VMEM((128, 128), F32),
        pltpu.VMEM((80, 128), BF),
        pltpu.VMEM((80, 128), BF),
        pltpu.VMEM((4, 80, 128), BF),
        pltpu.VMEM((nz // 4, 80, 128), BF),
        pltpu.VMEM((64, 128), BF),
        pltpu.VMEM((64, 128), BF),
        pltpu.VMEM((64, 128), F32),
        pltpu.VMEM((tokens, 128), F32),
        pltpu.VMEM((tokens, 128), F32),
        pltpu.VMEM((tokens, 128), F32),
        pltpu.VMEM((experts * cap, tokens), BF),
        pltpu.VMEM((2, tokens, experts * cap), BF),
        pltpu.VMEM((2, tokens, 128), F32),
        pltpu.VMEM((ny, nx, 2, 2, half // 2, 128), BF),
        pltpu.VMEM((2, 3, 4, 2, half // 2, 128), BF),
        pltpu.VMEM((2, 4, 2, half // 2, 128), BF),
        pltpu.VMEM((2, 3, 2, half // 2, 128), BF),
        pltpu.VMEM((experts, *block), BF),
        pltpu.VMEM((ny, 2, nz, *block), BF),
        pltpu.VMEM((ny, nx, nc, nz, *block), BF),
        pltpu.VMEM((nc * CHUNK * cap, width), BF),
        pltpu.VMEM((ny, nx, nc, nz, *block), BF),
        pltpu.VMEM((ny, nx, nz, *block), BF),
        pltpu.VMEM((ny, nx, nz, *block), BF),
        pltpu.VMEM((3, 4, nz, *block), BF),
        pltpu.VMEM((4, nz, *block), BF),
        pltpu.VMEM((4, 2, nz, *block), BF),
        pltpu.VMEM((3, nz, *block), BF),
        pltpu.VMEM((3, 2, nz, *block), BF),
        pltpu.VMEM((2, nz, *block), BF),
        pltpu.VMEM((experts, *block), BF),
        pltpu.SemaphoreType.DMA((16,)),
        pltpu.SemaphoreType.DMA((count,)),
        pltpu.SemaphoreType.DMA((count,)),
    ]
    return pl.pallas_call(
        functools.partial(kernel, sizes),
        out_shape=jax.ShapeDtypeStruct((tokens, 128), BF),
        in_specs=[anywhere] * 16,
        out_specs=vmem,
        scratch_shapes=scratch,
        compiler_params=pltpu.CompilerParams(collective_id=0, has_side_effects=True),
    )(
        asker_raw_scores,
        retain_raw_scores,
        memory_write_entries,
        emit_switch_scores,
        retain_minimum_share.reshape(1, 128),
        extra_shrink_rate,
        lane_rescale_factor.reshape(1, 128),
        specialist_rescale_factor.reshape(1, width),
        specialist_choice_ids.T,
        cluster_chance.reshape(1, tokens),
        specialist_duo_scores.T,
        skip_path_vectors,
        emit_projection_array,
        specialist_switch_proj[0],
        specialist_raise_proj[0],
        specialist_lower_proj[0],
    )


def solution(mesh, shape=(16, 2, 4, 4), tokens=256, cap=24):
    finer = Mesh(mesh.devices.reshape(shape), AXES)
    in_specs = (
        P(SP, None),
        P(SP, TP),
        P(SP, TP),
        P(SP, TP),
        P(SP, TP),
        P(TP),
        P(TP, SP),
        P(),
        P(TP, None),
        P(),
        P(SP, None, TP),
        P(SP, None, TP),
        P(SP, TP, None),
        P(SP, None),
        P(SP),
        P(SP, None),
    )
    return jax.shard_map(
        functools.partial(layer, (*shape, tokens, cap)),
        mesh=finer,
        in_specs=in_specs,
        out_specs=P(SP, TP),
        check_vma=False,
    )
```

```python
import functools

import jax
import jax.numpy as jnp
from jax import lax
from jax.experimental import pallas as pl
from jax.experimental.pallas import tpu as pltpu
from jax.sharding import Mesh
from jax.sharding import PartitionSpec as P

AXES = ("z", "c", "y", "x")
SP = ("z", "c")
TP = ("y", "x")
EPS = 1e-06
BF = jnp.bfloat16
F32 = jnp.float32
HIGH = lax.Precision.HIGHEST
MESH = pl.DeviceIdType.MESH
TILE = 8
CHUNK = 4


def dims_of(a, b, left, right, precision=None):
    return lax.dot_general(
        a, b, (((left,), (right,)), ((), ())), precision=precision, preferred_element_type=F32
    )


def z_steps(count):
    steps = [0]
    for far in range(1, count // 2 + 1):
        steps += [far, -far]
    steps = steps[:count]
    return steps[4:] + steps[:4] if count > 4 else steps


def column_of(row, eye):
    return jnp.sum(jnp.where(eye, row, 0.0), axis=1, keepdims=True)


class Wire:
    def __init__(self, sends, recvs):
        self.sends, self.recvs, self.used, self.started = sends, recvs, 0, []

    def slots(self, count):
        first = self.used
        self.used += count
        return first

    def copy(self, src, dst, number, device):
        return pltpu.make_async_remote_copy(
            src_ref=src,
            dst_ref=dst,
            send_sem=self.sends.at[number],
            recv_sem=self.recvs.at[number],
            device_id=device,
            device_id_type=MESH,
        )

    def send(self, src, dst, number, device):
        copy = self.copy(src, dst, number, device)
        copy.start()
        self.started.append(copy)

    def arrived(self, dst, number, device):
        self.copy(dst, dst, number, device).wait_recv()


def semaphore_count(nz, nc, tp):
    return 1 + 3 + 3 + 1 + 6 + 12 + 2 * nz + 26 * (nz // CHUNK)


def kernel(
    sizes,
    asker_hbm,
    retain_hbm,
    entries_hbm,
    emit_hbm,
    least_hbm,
    extra_hbm,
    lane_gain_hbm,
    row_gain_hbm,
    ids_hbm,
    chance_hbm,
    duo_hbm,
    skip_hbm,
    project_hbm,
    switch_hbm,
    raise_hbm,
    lower_hbm,
    out,
    asker,
    retain,
    entries,
    emit,
    least,
    extra,
    lane_gain,
    row_gain,
    ids,
    chance,
    duo,
    skip,
    project,
    switch,
    raised,
    lower,
    away_switch,
    away_raised,
    away_lower,
    state_own,
    state_first,
    half_out,
    half_in,
    near,
    far,
    back_out,
    back_in,
    prefix,
    query_hat,
    inside,
    gates,
    select_in,
    select_out,
    route,
    mix_part,
    mix_one,
    mix_sum,
    mix_three,
    slots,
    bands,
    rows,
    normed,
    part,
    other_part,
    summed,
    red_one,
    red_a,
    red_b,
    last_a,
    last_b,
    finished,
    returned,
    local_sems,
    sends,
    recvs,
):
    nz, nc, ny, nx, tokens, cap = sizes
    tp = ny * nx
    groups = nz // 4
    half = tokens // 2
    z, c, y, x = (lax.axis_index(a) for a in AXES)
    me_sp = z * nc + c
    wire = Wire(sends, recvs)
    steps = z_steps(nz)
    chunks = nz // CHUNK
    mine_expert = lax.rem(x, 2)
    keeps = c == mine_expert

    def device(dz=0, dc=0, dy=0, dx=0):
        return (
            lax.rem(z + (dz + nz), nz),
            lax.rem(c + dc, nc),
            lax.rem(y + (dy + ny), ny),
            lax.rem(x + (dx + nx), nx),
        )

    partner = device(dc=1)
    barrier = pltpu.get_barrier_semaphore()
    peers = [partner] + [device(dz=dz) for dz in steps if dz != 0]
    peers += [device(dy=d) for d in (1, -1, 2)] + [device(dx=d) for d in (1, -1, 2)]
    peers += [device(dx=d, dc=1) for d in (1, -1)]
    for peer in peers:
        pl.semaphore_signal(barrier, inc=1, device_id=peer, device_id_type=MESH)

    my_cols = pl.ds(pl.multiple_of((y * nx + x) * 128, 128), 128)
    loads = [
        pltpu.make_async_copy(src, dst, local_sems.at[i])
        for i, (src, dst) in enumerate(
            [
                (retain_hbm, retain),
                (least_hbm, least),
                (extra_hbm, extra),
                (entries_hbm, entries),
                (asker_hbm, asker),
                (emit_hbm, emit),
                (lane_gain_hbm, lane_gain),
                (ids_hbm, ids),
                (chance_hbm, chance),
                (duo_hbm, duo),
                (project_hbm, project),
                (skip_hbm.at[:, my_cols], skip),
                (row_gain_hbm, row_gain),
            ]
        )
    ]
    for load in loads:
        load.start()
    own_weights = [
        pltpu.make_async_copy(src, dst, local_sems.at[13 + i])
        for i, (src, dst) in enumerate(
            [(switch_hbm, switch), (raise_hbm, raised), (lower_hbm, lower)]
        )
    ]

    staged = [
        pltpu.make_async_copy(src, dst, local_sems.at[16 + i])
        for i, (src, dst) in enumerate(
            [(switch_hbm, away_switch), (raise_hbm, away_raised), (lower_hbm, away_lower)]
        )
    ]

    @pl.when(keeps)
    def _():
        for load in own_weights:
            load.start()

    @pl.when(jnp.logical_not(keeps))
    def _():
        for load in staged:
            load.start()

    for load in loads[:4]:
        load.wait()

    spots = lax.broadcasted_iota(jnp.int32, (half, half), 0)
    other = lax.broadcasted_iota(jnp.int32, (half, half), 1)
    causal = spots >= other
    causal_ones = jnp.where(causal, 1.0, 0.0).astype(F32)
    eye_half = spots == other

    def decays(b):
        mine = pl.ds(b * half, half)
        floor = least[...]
        share = floor + (1.0 - floor) * jax.nn.sigmoid(retain[mine, :].astype(F32))
        logs = jnp.log(share) + column_of(extra[:, b * half : (b + 1) * half], eye_half)
        total = jnp.dot(causal_ones, logs, precision=HIGH, preferred_element_type=F32)
        return total, 1.0 - share

    states, lasts, kept = [], [], []
    for b in range(2):
        total, keys = decays(b)
        last = total[half - 1 : half, :]
        ending = keys * jnp.exp(last - total)
        values = entries[b * half : (b + 1) * half, :].astype(F32)
        states.append(dims_of(values, ending, 0, 0, HIGH))
        lasts.append(last)
        kept.append((total, keys))
    own_decay = jnp.exp(lasts[0] + lasts[1])
    state_first[...] = states[0]
    state_own[...] = jnp.exp(lasts[1]) * states[0] + states[1]

    tail_row = lax.broadcasted_iota(jnp.int32, (16, 128), 0)

    def pack(ref, value, decay):
        top = decay.astype(BF)
        low = (decay - top.astype(F32)).astype(BF)
        ref[0:64, :] = value.astype(BF)
        tail = jnp.where(
            tail_row == 0, top.astype(F32), jnp.where(tail_row == 1, low.astype(F32), 0.0)
        )
        ref[64:80, :] = tail.astype(BF)

    def unpack(ref):
        tail = ref[64:80, :].astype(F32)
        return ref[0:64, :].astype(F32), tail[0:1, :] + tail[1:2, :]

    first_core = c == 0
    mine_half = jnp.where(first_core, state_own[0:64, :], state_own[64:128, :])
    theirs_half = jnp.where(first_core, state_own[64:128, :], state_own[0:64, :])
    pack(half_out, theirs_half, own_decay)

    pl.semaphore_wait(barrier, len(peers))

    for load in loads[4:10]:
        load.wait()
    n_half = wire.slots(1)
    n_near = wire.slots(3)
    n_far = wire.slots(3)
    n_back = wire.slots(1)
    wire.send(half_out, half_in, n_half, partner)

    n_weights = wire.slots(6)
    part_width = switch.shape[1] // 2

    def moved(way, delta):
        cut = slice(way * part_width, (way + 1) * part_width)
        refs = [
            (away_switch.at[:, cut], switch.at[:, cut]),
            (away_raised.at[:, cut], raised.at[:, cut]),
            (away_lower.at[cut, :], lower.at[cut, :]),
        ]
        there = device(dx=delta, dc=1)
        return [
            wire.copy(src, dst, n_weights + 3 * way + i, there) for i, (src, dst) in enumerate(refs)
        ]

    right_ones, left_ones = moved(0, 1), moved(1, -1)
    early, late = right_ones[:2] + left_ones[:2], [right_ones[2], left_ones[2]]

    @pl.when(jnp.logical_not(keeps))
    def _():
        for load in staged:
            load.wait()
        for copy in early:
            copy.start()


    def score_block(b):
        total, keys = kept[b]
        mine = pl.ds(b * half, half)
        middle = total[half // 2 - 1 : half // 2, :]
        asked = jax.nn.silu(asker[mine, :].astype(F32))
        query_hat[mine, :] = asked * jnp.exp(total)
        scores = dims_of(
            asked * jnp.exp(total - middle), keys * jnp.exp(middle - total), 1, 1, HIGH
        )
        scores = jnp.where(causal, scores, 0.0)
        values = entries[mine, :].astype(F32)
        inside[mine, :] = jnp.dot(scores, values, precision=HIGH, preferred_element_type=F32)
        gates[mine, :] = lane_gain[...] * jax.nn.silu(emit[mine, :].astype(F32))

    wire.arrived(half_in, n_half, partner)
    theirs, their_decay = unpack(half_in)
    s0 = jnp.where(first_core, mine_half, theirs)
    s1 = jnp.where(first_core, theirs, mine_half)
    d0 = jnp.where(first_core, own_decay, their_decay)
    d1 = jnp.where(first_core, their_decay, own_decay)
    group, place = z // 4, lax.rem(z, 4)
    pack(near.at[place], d1 * s0 + s1, d0 * d1)

    def in_group(j):
        return (group * 4 + lax.rem(place + j, 4), c, y, x)

    for j in (1, 2, 3):
        wire.send(near.at[place], near.at[place], n_near + j - 1, in_group(j))

    score_block(0)
    score_block(1)

    for j in (1, 2, 3):
        sender = lax.rem(place + 4 - j, 4)
        wire.arrived(near.at[sender], n_near + j - 1, in_group(4 - j))
    before = jnp.zeros((64, 128), F32)
    before_decay = jnp.ones((1, 128), F32)
    total_state, total_decay = before, before_decay
    for j in range(4):
        value, decay = unpack(near.at[j])
        total_state = decay * total_state + value
        total_decay = decay * total_decay
        earlier = j < place
        before = jnp.where(earlier, decay * before + value, before)
        before_decay = jnp.where(earlier, decay * before_decay, before_decay)
    pack(far.at[group], total_state, total_decay)

    def to_group(j):
        return (lax.rem(z + 4 * j, nz), c, y, x)

    for j in range(1, groups):

        @pl.when(group + j < groups)
        def _():
            wire.copy(far.at[group], far.at[group], n_far + j - 1, to_group(j)).start()

    tok_row = lax.broadcasted_iota(jnp.int32, (tokens, tokens), 0)
    tok_col = lax.broadcasted_iota(jnp.int32, (tokens, tokens), 1)
    eye = tok_row == tok_col
    earlier_ones = jnp.where(tok_row < tok_col, 1.0, 0.0).astype(BF)
    experts = nz * nc
    expert_at = lax.broadcasted_iota(jnp.int32, (experts, tokens), 0)
    named = [jnp.where(expert_at == ids[j : j + 1, :], 1.0, 0.0).astype(F32) for j in range(2)]
    counts = jnp.dot(
        (named[0] + named[1]).astype(BF), earlier_ones, preferred_element_type=F32
    )
    slot_rows = [
        ids[j : j + 1, :].astype(F32) * cap + jnp.sum(counts * named[j], axis=0, keepdims=True)
        for j in range(2)
    ]
    slot_at = lax.broadcasted_iota(jnp.int32, (experts * cap, tokens), 0).astype(F32)
    select_in[...] = jnp.where(
        slot_at == slot_rows[0], 1.0, jnp.where(slot_at == slot_rows[1], 1.0, 0.0)
    ).astype(BF)
    slot_along = lax.broadcasted_iota(jnp.int32, (tokens, experts * cap), 1).astype(F32)
    spread = duo[0:1, :] - duo[1:2, :]
    for j in range(2):
        select_out[j] = jnp.where(
            slot_along == column_of(slot_rows[j], eye), 1.0, 0.0
        ).astype(BF)
        weight = chance[...] * jax.nn.sigmoid(spread if j == 0 else -spread)
        route[j] = jnp.broadcast_to(column_of(weight, eye), (tokens, 128))

    prefix[...] = jnp.zeros((64, 128), F32)
    for j in range(groups - 1):

        @pl.when(j < group)
        def _():
            sender = j
            number = n_far + group - 1 - j
            wire.arrived(far.at[sender], number, to_group(0))
            value, decay = unpack(far.at[sender])
            prefix[...] = decay * prefix[...] + value

    start = before_decay * prefix[...] + before
    after_first = d0 * start + s0
    back_out[...] = jnp.where(first_core, after_first, start).astype(BF)
    wire.send(back_out, back_in, n_back, partner)
    own_start = jnp.where(first_core, start, after_first)
    wire.arrived(back_in, n_back, partner)
    got = back_in[...].astype(F32)
    carried = jnp.concatenate(
        [jnp.where(first_core, own_start, got), jnp.where(first_core, got, own_start)], axis=0
    )
    for j in range(1, groups):

        @pl.when(group + j < groups)
        def _():
            wire.copy(far.at[group], far.at[group], n_far + j - 1, to_group(j)).wait_send()

    second = jnp.exp(lasts[0]) * carried + state_first[...]
    loads[10].wait()
    for b, state in enumerate((carried, second)):
        mine = pl.ds(b * half, half)
        readout = inside[mine, :] + dims_of(query_hat[mine, :], state, 1, 1, HIGH)
        mean = jnp.mean(readout * readout, axis=1, keepdims=True)
        mixed = (readout * lax.rsqrt(mean + EPS) * gates[mine, :]).astype(BF)
        for t in range(0, tp, 2):
            wide = jnp.dot(
                mixed, project[:, t * 128 : (t + 2) * 128], preferred_element_type=F32
            )
            for u in range(t, min(t + 2, tp)):
                mix_part[u // nx, u % nx, b] = (
                    wide[:, (u - t) * 128 : (u - t + 1) * 128]
                    .reshape(2, half // 2, 128)
                    .astype(BF)
                )

    ways = (2, 1, -1)

    class Reduce:
        def __init__(self, source, lo, n, one, total, three):
            self.source, self.one, self.total, self.three = source, one, total, three
            self.first = wire.slots(12)
            self.span = pl.ds(lo, n)
            self.every = pl.ds(0, 4)

        def at(self, k, f, g):
            rest = (k, self.span)
            return self.source.at[(f, g) + rest] if k == 0 else self.source.at[(g, f) + rest]

        def axes(self, k):
            f, g = (y, x) if k == 0 else (x, y)
            name_f, name_g = ("dy", "dx") if k == 0 else ("dx", "dy")
            return f, g, (lambda d: device(**{name_f: d})), (lambda d: device(**{name_g: d}))

        def step_one(self):
            for k in range(2):
                f, g, to_f, to_g = self.axes(k)
                for way, delta in enumerate(ways):
                    wire.send(
                        self.at(k, lax.rem(f + delta + 4, 4), self.every),
                        self.one.at[k, way, self.every, self.span],
                        self.first + k * 6 + way,
                        to_f(delta),
                    )

        def step_three(self):
            for k in range(2):
                f, g, to_f, to_g = self.axes(k)
                value = self.at(k, f, self.every)[...].astype(F32)
                for way, delta in enumerate(ways):
                    came = self.one.at[k, way, self.every, self.span]
                    wire.arrived(came, self.first + k * 6 + way, to_f(-delta))
                    value = value + came[...].astype(F32)
                self.total[k, self.every, self.span] = value.astype(BF)
            for k in range(2):
                f, g, to_f, to_g = self.axes(k)
                for way, delta in enumerate(ways):
                    wire.send(
                        self.total.at[k, lax.rem(g + delta + 4, 4), self.span],
                        self.three.at[k, way, self.span],
                        self.first + k * 6 + 3 + way,
                        to_g(delta),
                    )

        def result(self, k):
            f, g, to_f, to_g = self.axes(k)
            value = self.at(k, f, g)[...].astype(F32)
            for way, delta in enumerate(ways):
                value = value + self.one[k, way, g, self.span].astype(F32)
            for way, delta in enumerate(ways):
                came = self.three.at[k, way, self.span]
                wire.arrived(came, self.first + k * 6 + 3 + way, to_g(-delta))
                value = value + came[...].astype(F32)
            return value

    loads[11].wait()
    if tp > 1:
        mix = Reduce(mix_part, 0, 2, mix_one, mix_sum, mix_three)
        mix.step_one()
        mix.step_three()
        own_cols = [mix.result(k).reshape(half, 128) for k in range(2)]
    else:
        own_cols = [mix_part[0, 0, k].astype(F32).reshape(half, 128) for k in range(2)]
    for k in range(2):
        mine = pl.ds(k * half, half)
        skip[mine, :] = (skip[mine, :].astype(F32) + own_cols[k]).astype(BF)

    @pl.when(jnp.logical_not(keeps))
    def _():
        for copy in late:
            copy.start()

    tiles = cap // TILE
    slots[...] = (
        jnp.dot(select_in[...], skip[...], preferred_element_type=F32)
        .reshape(experts, tiles, TILE, 128)
        .astype(BF)
    )
    n_out = wire.slots(nz)
    bands[y, :, steps.index(0)] = slots[pl.ds(2 * z, 2)]
    for i, dz in enumerate(steps):
        if dz == 0:
            continue
        there = device(dz=dz)
        wire.send(
            slots.at[pl.ds(2 * there[0], 2)], bands.at[y, :, i], n_out + i, there
        )

    four = pl.ds(0, 4)

    class Chunk:
        def __init__(self, number):
            self.lo = number * CHUNK
            self.h = CHUNK // 2
            self.first = wire.slots(26)
            self.whole = pl.ds(self.lo, CHUNK)
            self.spans = [pl.ds(self.lo, self.h), pl.ds(self.lo + self.h, self.h)]

        def expert_for(self, delta):
            return mine_expert if delta == 2 else 1 - mine_expert

        def gather_one(self):
            for i in range(self.lo, self.lo + CHUNK):
                if steps[i] != 0:
                    wire.arrived(bands.at[y, :, i], n_out + i, device(dz=-steps[i]))
            a, b = self.spans
            for way, delta in enumerate(ways):
                wire.send(
                    bands.at[y, self.expert_for(delta), a],
                    rows.at[y, x, c, a],
                    self.first + way,
                    device(dx=delta),
                )
                both = bands.at[y, pl.ds(0, 2), b]
                wire.send(both, both, self.first + 3 + way, device(dy=delta))
            rows[y, x, c, a] = bands[y, mine_expert, a]

        def gather_two(self):
            a, b = self.spans
            for way, delta in enumerate(ways):
                came_x = lax.rem(x - delta + 4, 4)
                wire.arrived(rows.at[y, came_x, c, a], self.first + way, device(dx=-delta))
            for way, delta in enumerate(ways):
                quad = rows.at[y, four, c, a]
                wire.send(quad, quad, self.first + 6 + way, device(dy=delta))
            for way, delta in enumerate(ways):
                came_y = lax.rem(y - delta + 4, 4)
                wire.arrived(
                    bands.at[came_y, pl.ds(0, 2), b], self.first + 3 + way, device(dy=-delta)
                )
            for way, delta in enumerate(ways):
                wire.send(
                    bands.at[four, self.expert_for(delta), b],
                    rows.at[four, x, c, b],
                    self.first + 9 + way,
                    device(dx=delta),
                )
            rows[four, x, c, b] = bands[four, mine_expert, b]

        def gather_three(self):
            a, b = self.spans
            for way, delta in enumerate(ways):
                came_x, came_y = lax.rem(x - delta + 4, 4), lax.rem(y - delta + 4, 4)
                wire.arrived(
                    rows.at[came_y, four, c, a], self.first + 6 + way, device(dy=-delta)
                )
                wire.arrived(
                    rows.at[four, came_x, c, b], self.first + 9 + way, device(dx=-delta)
                )
            mine = rows.at[four, four, c, self.whole]
            wire.send(mine, mine, self.first + 12, partner)

        def experts(self):
            wire.arrived(rows.at[four, four, 1 - c, self.whole], self.first + 12, partner)
            if self.lo == 0:
                weights_are_here()
            count = nc * CHUNK * cap
            squares = jnp.zeros((count, 128), F32)
            for t in range(tp):
                wide = rows[t // nx, t % nx, :, self.whole].astype(F32).reshape(count, 128)
                squares = squares + wide * wide
            scale = lax.rsqrt(jnp.sum(squares, axis=1, keepdims=True) / (tp * 128) + EPS)
            for t in range(tp):
                wide = rows[t // nx, t % nx, :, self.whole].astype(F32).reshape(count, 128)
                cols = slice(t * 128, (t + 1) * 128)
                normed[:, cols] = (wide * scale * row_gain[:, cols]).astype(BF)
            gate_acts = jnp.dot(normed[...], switch[...], preferred_element_type=F32)
            up_acts = jnp.dot(normed[...], raised[...], preferred_element_type=F32)
            hidden = (jax.nn.silu(gate_acts) * up_acts).astype(BF)
            for t in range(0, tp, 2):
                wide = jnp.dot(
                    hidden, lower[:, t * 128 : (t + 2) * 128], preferred_element_type=F32
                )
                for u in range(t, t + 2):
                    part[u // nx, u % nx, :, self.whole] = (
                        wide[:, (u - t) * 128 : (u - t + 1) * 128]
                        .reshape(nc, CHUNK, tiles, TILE, 128)
                        .astype(BF)
                    )
            wire.send(
                part.at[four, four, 1 - c, self.whole],
                other_part.at[four, four, self.whole],
                self.first + 13,
                partner,
            )

        def sum_one(self):
            came = other_part.at[four, four, self.whole]
            wire.arrived(came, self.first + 13, partner)
            for t in range(tp):
                at = (t // nx, t % nx)
                summed[at[0], at[1], self.whole] = (
                    part[at[0], at[1], c, self.whole].astype(F32)
                    + other_part[at[0], at[1], self.whole].astype(F32)
                ).astype(BF)
            a, b = self.spans
            for way, delta in enumerate(ways):
                to_y, to_x = lax.rem(y + delta + 4, 4), lax.rem(x + delta + 4, 4)
                wire.send(
                    summed.at[to_y, four, a],
                    red_one.at[way, four, a],
                    self.first + 14 + way,
                    device(dy=delta),
                )
                wire.send(
                    summed.at[four, to_x, b],
                    red_one.at[way, four, b],
                    self.first + 17 + way,
                    device(dx=delta),
                )

        def first_sum(self, index):
            a = self.spans[0]
            value = summed[y, index, a].astype(F32)
            for way in range(3):
                value = value + red_one[way, index, a].astype(F32)
            return value

        def second_sums(self, index):
            b = self.spans[1]
            own = summed[index, x, b].astype(F32) + red_one[0, index, b].astype(F32)
            return own, red_one[1, index, b].astype(F32) + red_one[2, index, b].astype(F32)

        def sum_two(self):
            a, b = self.spans
            for way, delta in enumerate(ways):
                wire.arrived(
                    red_one.at[way, four, a], self.first + 14 + way, device(dy=-delta)
                )
                wire.arrived(
                    red_one.at[way, four, b], self.first + 17 + way, device(dx=-delta)
                )
            red_a[four, a] = self.first_sum(four).astype(BF)
            own, other = self.second_sums(four)
            red_b[four, mine_expert, b] = own.astype(BF)
            red_b[four, 1 - mine_expert, b] = other.astype(BF)
            for way, delta in enumerate(ways):
                to_y, to_x = lax.rem(y + delta + 4, 4), lax.rem(x + delta + 4, 4)
                wire.send(
                    red_a.at[to_x, a],
                    last_a.at[way, a],
                    self.first + 20 + way,
                    device(dx=delta),
                )
                wire.send(
                    red_b.at[to_y, pl.ds(0, 2), b],
                    last_b.at[way, pl.ds(0, 2), b],
                    self.first + 23 + way,
                    device(dy=delta),
                )

        def give_back(self):
            a, b = self.spans
            for way, delta in enumerate(ways):
                wire.arrived(last_a.at[way, a], self.first + 20 + way, device(dx=-delta))
                wire.arrived(
                    last_b.at[way, pl.ds(0, 2), b], self.first + 23 + way, device(dy=-delta)
                )
            finished[mine_expert, a] = (
                self.first_sum(x) + last_a[0, a].astype(F32)
            ).astype(BF)
            finished[1 - mine_expert, a] = (
                last_a[1, a].astype(F32) + last_a[2, a].astype(F32)
            ).astype(BF)
            own, other = self.second_sums(y)
            for expert, value in ((mine_expert, own), (1 - mine_expert, other)):
                for way in range(3):
                    value = value + last_b[way, expert, b].astype(F32)
                finished[expert, b] = value.astype(BF)
            for i in range(self.lo, self.lo + CHUNK):
                if steps[i] == 0:
                    returned[pl.ds(2 * z, 2)] = finished[:, i]
                    continue
                wire.send(
                    finished.at[pl.ds(0, 2), i],
                    returned.at[pl.ds(2 * z, 2)],
                    n_home + i,
                    device(dz=-steps[i]),
                )

    n_home = wire.slots(nz)
    work = [Chunk(n) for n in range(chunks)]
    loads[12].wait()

    def weights_are_here():
        @pl.when(keeps)
        def _():
            for load in own_weights:
                load.wait()

        @pl.when(jnp.logical_not(keeps))
        def _():
            for copy in early + late:
                copy.wait_send()
                copy.wait_recv()

    order = (
        "gather_one",
        "gather_two",
        "gather_three",
        "experts",
        "sum_one",
        "sum_two",
        "give_back",
    )
    at = (0, 3, 7, 9, 11, 15, 19)
    tasks = sorted((at[j] + 2.2 * n, n, j) for n in range(chunks) for j in range(len(order)))
    for _, n, j in tasks:
        getattr(work[n], order[j])()

    for i, dz in enumerate(steps):
        if dz != 0:
            there = device(dz=dz)
            wire.arrived(returned.at[pl.ds(2 * there[0], 2)], n_home + i, there)
    got_rows = returned[...].astype(F32).reshape(experts * cap, 128).astype(BF)
    result = skip[...].astype(F32)
    for j in range(2):
        picked = jnp.dot(select_out[j], got_rows, preferred_element_type=F32)
        result = result + route[j] * picked
    out[...] = result.astype(BF)
    for copy in wire.started:
        copy.wait_send()


def layer(
    sizes,
    skip_path_vectors,
    asker_raw_scores,
    retain_raw_scores,
    memory_write_entries,
    emit_switch_scores,
    retain_minimum_share,
    extra_shrink_rate,
    lane_rescale_factor,
    emit_projection_array,
    specialist_rescale_factor,
    specialist_switch_proj,
    specialist_raise_proj,
    specialist_lower_proj,
    specialist_choice_ids,
    cluster_chance,
    specialist_duo_scores,
):
    nz, nc, ny, nx, tokens, cap = sizes
    tp = ny * nx
    width = tp * 128
    hidden = specialist_switch_proj.shape[2]
    half, experts, tiles = tokens // 2, nz * nc, cap // TILE
    block = (tiles, TILE, 128)
    vmem, anywhere = (
        pl.BlockSpec(memory_space=pltpu.VMEM),
        pl.BlockSpec(memory_space=pl.ANY),
    )
    count = semaphore_count(nz, nc, tp)
    scratch = [
        pltpu.VMEM((tokens, 128), BF),
        pltpu.VMEM((tokens, 128), BF),
        pltpu.VMEM((tokens, 128), BF),
        pltpu.VMEM((tokens, 128), BF),
        pltpu.VMEM((1, 128), F32),
        pltpu.VMEM((1, tokens), F32),
        pltpu.VMEM((1, 128), F32),
        pltpu.VMEM((1, width), F32),
        pltpu.VMEM((2, tokens), jnp.int32),
        pltpu.VMEM((1, tokens), F32),
        pltpu.VMEM((2, tokens), F32),
        pltpu.VMEM((tokens, 128), BF),
        pltpu.VMEM((128, width), BF),
        pltpu.VMEM((width, hidden), BF),
        pltpu.VMEM((width, hidden), BF),
        pltpu.VMEM((hidden, width), BF),
        pltpu.VMEM((width, hidden), BF),
        pltpu.VMEM((width, hidden), BF),
        pltpu.VMEM((hidden, width), BF),
        pltpu.VMEM((128, 128), F32),
        pltpu.VMEM((128, 128), F32),
        pltpu.VMEM((80, 128), BF),
        pltpu.VMEM((80, 128), BF),
        pltpu.VMEM((4, 80, 128), BF),
        pltpu.VMEM((nz // 4, 80, 128), BF),
        pltpu.VMEM((64, 128), BF),
        pltpu.VMEM((64, 128), BF),
        pltpu.VMEM((64, 128), F32),
        pltpu.VMEM((tokens, 128), F32),
        pltpu.VMEM((tokens, 128), F32),
        pltpu.VMEM((tokens, 128), F32),
        pltpu.VMEM((experts * cap, tokens), BF),
        pltpu.VMEM((2, tokens, experts * cap), BF),
        pltpu.VMEM((2, tokens, 128), F32),
        pltpu.VMEM((ny, nx, 2, 2, half // 2, 128), BF),
        pltpu.VMEM((2, 3, 4, 2, half // 2, 128), BF),
        pltpu.VMEM((2, 4, 2, half // 2, 128), BF),
        pltpu.VMEM((2, 3, 2, half // 2, 128), BF),
        pltpu.VMEM((experts, *block), BF),
        pltpu.VMEM((ny, 2, nz, *block), BF),
        pltpu.VMEM((ny, nx, nc, nz, *block), BF),
        pltpu.VMEM((nc * CHUNK * cap, width), BF),
        pltpu.VMEM((ny, nx, nc, nz, *block), BF),
        pltpu.VMEM((ny, nx, nz, *block), BF),
        pltpu.VMEM((ny, nx, nz, *block), BF),
        pltpu.VMEM((3, 4, nz, *block), BF),
        pltpu.VMEM((4, nz, *block), BF),
        pltpu.VMEM((4, 2, nz, *block), BF),
        pltpu.VMEM((3, nz, *block), BF),
        pltpu.VMEM((3, 2, nz, *block), BF),
        pltpu.VMEM((2, nz, *block), BF),
        pltpu.VMEM((experts, *block), BF),
        pltpu.SemaphoreType.DMA((19,)),
        pltpu.SemaphoreType.DMA((count,)),
        pltpu.SemaphoreType.DMA((count,)),
    ]
    return pl.pallas_call(
        functools.partial(kernel, sizes),
        out_shape=jax.ShapeDtypeStruct((tokens, 128), BF),
        in_specs=[anywhere] * 16,
        out_specs=vmem,
        scratch_shapes=scratch,
        compiler_params=pltpu.CompilerParams(collective_id=0, has_side_effects=True),
    )(
        asker_raw_scores,
        retain_raw_scores,
        memory_write_entries,
        emit_switch_scores,
        retain_minimum_share.reshape(1, 128),
        extra_shrink_rate,
        lane_rescale_factor.reshape(1, 128),
        specialist_rescale_factor.reshape(1, width),
        specialist_choice_ids.T,
        cluster_chance.reshape(1, tokens),
        specialist_duo_scores.T,
        skip_path_vectors,
        emit_projection_array,
        specialist_switch_proj[0],
        specialist_raise_proj[0],
        specialist_lower_proj[0],
    )


def solution(mesh, shape=(16, 2, 4, 4), tokens=256, cap=24):
    finer = Mesh(mesh.devices.reshape(shape), AXES)
    in_specs = (
        P(SP, None),
        P(SP, TP),
        P(SP, TP),
        P(SP, TP),
        P(SP, TP),
        P(TP),
        P(TP, SP),
        P(),
        P(TP, None),
        P(),
        P(SP, None, TP),
        P(SP, None, TP),
        P(SP, TP, None),
        P(SP, None),
        P(SP),
        P(SP, None),
    )
    return jax.shard_map(
        functools.partial(layer, (*shape, tokens, cap)),
        mesh=finer,
        in_specs=in_specs,
        out_specs=P(SP, TP),
        check_vma=False,
    )
```

```python
import functools

import jax
import jax.numpy as jnp
from jax import lax
from jax.experimental import pallas as pl
from jax.experimental.pallas import tpu as pltpu
from jax.sharding import Mesh
from jax.sharding import PartitionSpec as P

AXES = ("z", "c", "y", "x")
SP = ("z", "c")
TP = ("y", "x")
EPS = 1e-06
BF = jnp.bfloat16
F32 = jnp.float32
HIGH = lax.Precision.HIGHEST
MESH = pl.DeviceIdType.MESH
TILE = 8
CHUNK = 4


def dims_of(a, b, left, right, precision=None):
    return lax.dot_general(
        a, b, (((left,), (right,)), ((), ())), precision=precision, preferred_element_type=F32
    )


def z_steps(count):
    steps = [0]
    for far in range(1, count // 2 + 1):
        steps += [far, -far]
    steps = steps[:count]
    return steps[4:] + steps[:4] if count > 4 else steps


def column_of(row, eye):
    return jnp.sum(jnp.where(eye, row, 0.0), axis=1, keepdims=True)


class Wire:
    def __init__(self, sends, recvs):
        self.sends, self.recvs, self.used, self.started = sends, recvs, 0, []

    def slots(self, count):
        first = self.used
        self.used += count
        return first

    def copy(self, src, dst, number, device):
        return pltpu.make_async_remote_copy(
            src_ref=src,
            dst_ref=dst,
            send_sem=self.sends.at[number],
            recv_sem=self.recvs.at[number],
            device_id=device,
            device_id_type=MESH,
        )

    def send(self, src, dst, number, device):
        copy = self.copy(src, dst, number, device)
        copy.start()
        self.started.append(copy)

    def arrived(self, dst, number, device):
        self.copy(dst, dst, number, device).wait_recv()


def semaphore_count(nz, nc, tp):
    return 1 + 3 + 3 + 1 + 6 + 12 + 2 * nz + 26 * (nz // CHUNK)


def kernel(
    sizes,
    asker_hbm,
    retain_hbm,
    entries_hbm,
    emit_hbm,
    least_hbm,
    extra_hbm,
    lane_gain_hbm,
    row_gain_hbm,
    ids_hbm,
    chance_hbm,
    duo_hbm,
    skip_hbm,
    project_hbm,
    switch_hbm,
    raise_hbm,
    lower_hbm,
    out,
    asker,
    retain,
    entries,
    emit,
    least,
    extra,
    lane_gain,
    row_gain,
    ids,
    chance,
    duo,
    skip,
    project,
    switch,
    raised,
    lower,
    away_switch,
    away_raised,
    away_lower,
    state_own,
    state_first,
    half_out,
    half_in,
    near,
    far,
    back_out,
    back_in,
    prefix,
    query_hat,
    inside,
    gates,
    select_in,
    select_out,
    route,
    mix_part,
    mix_one,
    mix_sum,
    mix_three,
    slots,
    bands,
    rows,
    normed,
    part,
    other_part,
    summed,
    red_one,
    red_a,
    red_b,
    last_a,
    last_b,
    finished,
    returned,
    local_sems,
    sends,
    recvs,
):
    nz, nc, ny, nx, tokens, cap = sizes
    tp = ny * nx
    groups = nz // 4
    half = tokens // 2
    z, c, y, x = (lax.axis_index(a) for a in AXES)
    me_sp = z * nc + c
    wire = Wire(sends, recvs)
    steps = z_steps(nz)
    chunks = nz // CHUNK
    mine_expert = lax.rem(x, 2)
    keeps = c == mine_expert

    def device(dz=0, dc=0, dy=0, dx=0):
        return (
            lax.rem(z + (dz + nz), nz),
            lax.rem(c + dc, nc),
            lax.rem(y + (dy + ny), ny),
            lax.rem(x + (dx + nx), nx),
        )

    partner = device(dc=1)
    barrier = pltpu.get_barrier_semaphore()
    peers = [partner] + [device(dz=dz) for dz in steps if dz != 0]
    peers += [device(dy=d) for d in (1, -1, 2)] + [device(dx=d) for d in (1, -1, 2)]
    peers += [device(dx=d, dc=1) for d in (1, -1)]
    for peer in peers:
        pl.semaphore_signal(barrier, inc=1, device_id=peer, device_id_type=MESH)

    my_cols = pl.ds(pl.multiple_of((y * nx + x) * 128, 128), 128)
    loads = [
        pltpu.make_async_copy(src, dst, local_sems.at[i])
        for i, (src, dst) in enumerate(
            [
                (retain_hbm, retain),
                (least_hbm, least),
                (extra_hbm, extra),
                (entries_hbm, entries),
                (asker_hbm, asker),
                (emit_hbm, emit),
                (lane_gain_hbm, lane_gain),
                (ids_hbm, ids),
                (chance_hbm, chance),
                (duo_hbm, duo),
                (project_hbm, project),
                (skip_hbm.at[:, my_cols], skip),
                (row_gain_hbm, row_gain),
            ]
        )
    ]
    for load in loads:
        load.start()
    own_weights = [
        pltpu.make_async_copy(src, dst, local_sems.at[13 + i])
        for i, (src, dst) in enumerate(
            [(switch_hbm, switch), (raise_hbm, raised), (lower_hbm, lower)]
        )
    ]

    staged = [
        pltpu.make_async_copy(src, dst, local_sems.at[16 + i])
        for i, (src, dst) in enumerate(
            [(switch_hbm, away_switch), (raise_hbm, away_raised), (lower_hbm, away_lower)]
        )
    ]

    @pl.when(keeps)
    def _():
        for load in own_weights:
            load.start()

    @pl.when(jnp.logical_not(keeps))
    def _():
        for load in staged:
            load.start()

    for load in loads[:4]:
        load.wait()

    spots = lax.broadcasted_iota(jnp.int32, (half, half), 0)
    other = lax.broadcasted_iota(jnp.int32, (half, half), 1)
    causal = spots >= other
    causal_ones = jnp.where(causal, 1.0, 0.0).astype(F32)
    eye_half = spots == other

    def decays(b):
        mine = pl.ds(b * half, half)
        floor = least[...]
        share = floor + (1.0 - floor) * jax.nn.sigmoid(retain[mine, :].astype(F32))
        logs = jnp.log(share) + column_of(extra[:, b * half : (b + 1) * half], eye_half)
        total = jnp.dot(causal_ones, logs, precision=HIGH, preferred_element_type=F32)
        return total, 1.0 - share

    states, lasts, kept = [], [], []
    for b in range(2):
        total, keys = decays(b)
        last = total[half - 1 : half, :]
        ending = keys * jnp.exp(last - total)
        values = entries[b * half : (b + 1) * half, :].astype(F32)
        states.append(dims_of(values, ending, 0, 0, HIGH))
        lasts.append(last)
        kept.append((total, keys))
    own_decay = jnp.exp(lasts[0] + lasts[1])
    state_first[...] = states[0]
    state_own[...] = jnp.exp(lasts[1]) * states[0] + states[1]

    tail_row = lax.broadcasted_iota(jnp.int32, (16, 128), 0)

    def pack(ref, value, decay):
        top = decay.astype(BF)
        low = (decay - top.astype(F32)).astype(BF)
        ref[0:64, :] = value.astype(BF)
        tail = jnp.where(
            tail_row == 0, top.astype(F32), jnp.where(tail_row == 1, low.astype(F32), 0.0)
        )
        ref[64:80, :] = tail.astype(BF)

    def unpack(ref):
        tail = ref[64:80, :].astype(F32)
        return ref[0:64, :].astype(F32), tail[0:1, :] + tail[1:2, :]

    first_core = c == 0
    mine_half = jnp.where(first_core, state_own[0:64, :], state_own[64:128, :])
    theirs_half = jnp.where(first_core, state_own[64:128, :], state_own[0:64, :])
    pack(half_out, theirs_half, own_decay)

    pl.semaphore_wait(barrier, len(peers))

    for load in loads[4:10]:
        load.wait()
    n_half = wire.slots(1)
    n_near = wire.slots(3)
    n_far = wire.slots(3)
    n_back = wire.slots(1)
    wire.send(half_out, half_in, n_half, partner)

    n_weights = wire.slots(6)
    part_width = switch.shape[1] // 2

    def moved(way, delta):
        cut = slice(way * part_width, (way + 1) * part_width)
        refs = [
            (away_switch.at[:, cut], switch.at[:, cut]),
            (away_raised.at[:, cut], raised.at[:, cut]),
            (away_lower.at[cut, :], lower.at[cut, :]),
        ]
        there = device(dx=delta, dc=1)
        return [
            wire.copy(src, dst, n_weights + 3 * way + i, there) for i, (src, dst) in enumerate(refs)
        ]

    right_ones, left_ones = moved(0, 1), moved(1, -1)
    early, late = right_ones[:2] + left_ones[:2], [right_ones[2], left_ones[2]]

    @pl.when(jnp.logical_not(keeps))
    def _():
        for load in staged:
            load.wait()
        for copy in early:
            copy.start()


    def score_block(b):
        total, keys = kept[b]
        mine = pl.ds(b * half, half)
        middle = total[half // 2 - 1 : half // 2, :]
        asked = jax.nn.silu(asker[mine, :].astype(F32))
        query_hat[mine, :] = asked * jnp.exp(total)
        scores = dims_of(
            asked * jnp.exp(total - middle), keys * jnp.exp(middle - total), 1, 1, HIGH
        )
        scores = jnp.where(causal, scores, 0.0)
        values = entries[mine, :].astype(F32)
        inside[mine, :] = jnp.dot(scores, values, precision=HIGH, preferred_element_type=F32)
        gates[mine, :] = lane_gain[...] * jax.nn.silu(emit[mine, :].astype(F32))

    wire.arrived(half_in, n_half, partner)
    theirs, their_decay = unpack(half_in)
    s0 = jnp.where(first_core, mine_half, theirs)
    s1 = jnp.where(first_core, theirs, mine_half)
    d0 = jnp.where(first_core, own_decay, their_decay)
    d1 = jnp.where(first_core, their_decay, own_decay)
    group, place = z // 4, lax.rem(z, 4)
    pack(near.at[place], d1 * s0 + s1, d0 * d1)

    def in_group(j):
        return (group * 4 + lax.rem(place + j, 4), c, y, x)

    for j in (1, 2, 3):
        wire.send(near.at[place], near.at[place], n_near + j - 1, in_group(j))

    score_block(0)
    score_block(1)

    for j in (1, 2, 3):
        sender = lax.rem(place + 4 - j, 4)
        wire.arrived(near.at[sender], n_near + j - 1, in_group(4 - j))
    before = jnp.zeros((64, 128), F32)
    before_decay = jnp.ones((1, 128), F32)
    total_state, total_decay = before, before_decay
    for j in range(4):
        value, decay = unpack(near.at[j])
        total_state = decay * total_state + value
        total_decay = decay * total_decay
        earlier = j < place
        before = jnp.where(earlier, decay * before + value, before)
        before_decay = jnp.where(earlier, decay * before_decay, before_decay)
    pack(far.at[group], total_state, total_decay)

    def to_group(j):
        return (lax.rem(z + 4 * j, nz), c, y, x)

    for j in range(1, groups):

        @pl.when(group + j < groups)
        def _():
            wire.copy(far.at[group], far.at[group], n_far + j - 1, to_group(j)).start()

    tok_row = lax.broadcasted_iota(jnp.int32, (tokens, tokens), 0)
    tok_col = lax.broadcasted_iota(jnp.int32, (tokens, tokens), 1)
    eye = tok_row == tok_col
    earlier_ones = jnp.where(tok_row < tok_col, 1.0, 0.0).astype(BF)
    experts = nz * nc
    expert_at = lax.broadcasted_iota(jnp.int32, (experts, tokens), 0)
    named = [jnp.where(expert_at == ids[j : j + 1, :], 1.0, 0.0).astype(F32) for j in range(2)]
    counts = jnp.dot(
        (named[0] + named[1]).astype(BF), earlier_ones, preferred_element_type=F32
    )
    slot_rows = [
        ids[j : j + 1, :].astype(F32) * cap + jnp.sum(counts * named[j], axis=0, keepdims=True)
        for j in range(2)
    ]
    slot_at = lax.broadcasted_iota(jnp.int32, (experts * cap, tokens), 0).astype(F32)
    select_in[...] = jnp.where(
        slot_at == slot_rows[0], 1.0, jnp.where(slot_at == slot_rows[1], 1.0, 0.0)
    ).astype(BF)
    slot_along = lax.broadcasted_iota(jnp.int32, (tokens, experts * cap), 1).astype(F32)
    spread = duo[0:1, :] - duo[1:2, :]
    for j in range(2):
        select_out[j] = jnp.where(
            slot_along == column_of(slot_rows[j], eye), 1.0, 0.0
        ).astype(BF)
        weight = chance[...] * jax.nn.sigmoid(spread if j == 0 else -spread)
        route[j] = jnp.broadcast_to(column_of(weight, eye), (tokens, 128))

    prefix[...] = jnp.zeros((64, 128), F32)
    for j in range(groups - 1):

        @pl.when(j < group)
        def _():
            sender = j
            number = n_far + group - 1 - j
            wire.arrived(far.at[sender], number, to_group(0))
            value, decay = unpack(far.at[sender])
            prefix[...] = decay * prefix[...] + value

    start = before_decay * prefix[...] + before
    after_first = d0 * start + s0
    back_out[...] = jnp.where(first_core, after_first, start).astype(BF)
    wire.send(back_out, back_in, n_back, partner)
    own_start = jnp.where(first_core, start, after_first)
    wire.arrived(back_in, n_back, partner)
    got = back_in[...].astype(F32)
    carried = jnp.concatenate(
        [jnp.where(first_core, own_start, got), jnp.where(first_core, got, own_start)], axis=0
    )
    for j in range(1, groups):

        @pl.when(group + j < groups)
        def _():
            wire.copy(far.at[group], far.at[group], n_far + j - 1, to_group(j)).wait_send()

    second = jnp.exp(lasts[0]) * carried + state_first[...]
    loads[10].wait()
    for b, state in enumerate((carried, second)):
        mine = pl.ds(b * half, half)
        readout = inside[mine, :] + dims_of(query_hat[mine, :], state, 1, 1)
        mean = jnp.mean(readout * readout, axis=1, keepdims=True)
        mixed = (readout * lax.rsqrt(mean + EPS) * gates[mine, :]).astype(BF)
        for t in range(0, tp, 2):
            wide = jnp.dot(
                mixed, project[:, t * 128 : (t + 2) * 128], preferred_element_type=F32
            )
            for u in range(t, min(t + 2, tp)):
                mix_part[u // nx, u % nx, b] = (
                    wide[:, (u - t) * 128 : (u - t + 1) * 128]
                    .reshape(2, half // 2, 128)
                    .astype(BF)
                )

    ways = (2, 1, -1)

    class Reduce:
        def __init__(self, source, lo, n, one, total, three):
            self.source, self.one, self.total, self.three = source, one, total, three
            self.first = wire.slots(12)
            self.span = pl.ds(lo, n)
            self.every = pl.ds(0, 4)

        def at(self, k, f, g):
            rest = (k, self.span)
            return self.source.at[(f, g) + rest] if k == 0 else self.source.at[(g, f) + rest]

        def axes(self, k):
            f, g = (y, x) if k == 0 else (x, y)
            name_f, name_g = ("dy", "dx") if k == 0 else ("dx", "dy")
            return f, g, (lambda d: device(**{name_f: d})), (lambda d: device(**{name_g: d}))

        def step_one(self):
            for k in range(2):
                f, g, to_f, to_g = self.axes(k)
                for way, delta in enumerate(ways):
                    wire.send(
                        self.at(k, lax.rem(f + delta + 4, 4), self.every),
                        self.one.at[k, way, self.every, self.span],
                        self.first + k * 6 + way,
                        to_f(delta),
                    )

        def step_three(self):
            for k in range(2):
                f, g, to_f, to_g = self.axes(k)
                value = self.at(k, f, self.every)[...].astype(F32)
                for way, delta in enumerate(ways):
                    came = self.one.at[k, way, self.every, self.span]
                    wire.arrived(came, self.first + k * 6 + way, to_f(-delta))
                    value = value + came[...].astype(F32)
                self.total[k, self.every, self.span] = value.astype(BF)
            for k in range(2):
                f, g, to_f, to_g = self.axes(k)
                for way, delta in enumerate(ways):
                    wire.send(
                        self.total.at[k, lax.rem(g + delta + 4, 4), self.span],
                        self.three.at[k, way, self.span],
                        self.first + k * 6 + 3 + way,
                        to_g(delta),
                    )

        def result(self, k):
            f, g, to_f, to_g = self.axes(k)
            value = self.at(k, f, g)[...].astype(F32)
            for way, delta in enumerate(ways):
                value = value + self.one[k, way, g, self.span].astype(F32)
            for way, delta in enumerate(ways):
                came = self.three.at[k, way, self.span]
                wire.arrived(came, self.first + k * 6 + 3 + way, to_g(-delta))
                value = value + came[...].astype(F32)
            return value

    loads[11].wait()
    if tp > 1:
        mix = Reduce(mix_part, 0, 2, mix_one, mix_sum, mix_three)
        mix.step_one()
        mix.step_three()
        own_cols = [mix.result(k).reshape(half, 128) for k in range(2)]
    else:
        own_cols = [mix_part[0, 0, k].astype(F32).reshape(half, 128) for k in range(2)]
    for k in range(2):
        mine = pl.ds(k * half, half)
        skip[mine, :] = (skip[mine, :].astype(F32) + own_cols[k]).astype(BF)

    @pl.when(jnp.logical_not(keeps))
    def _():
        for copy in late:
            copy.start()

    tiles = cap // TILE
    slots[...] = (
        jnp.dot(select_in[...], skip[...], preferred_element_type=F32)
        .reshape(experts, tiles, TILE, 128)
        .astype(BF)
    )
    n_out = wire.slots(nz)
    bands[y, :, steps.index(0)] = slots[pl.ds(2 * z, 2)]
    for i, dz in enumerate(steps):
        if dz == 0:
            continue
        there = device(dz=dz)
        wire.send(
            slots.at[pl.ds(2 * there[0], 2)], bands.at[y, :, i], n_out + i, there
        )

    four = pl.ds(0, 4)

    class Chunk:
        def __init__(self, number):
            self.lo = number * CHUNK
            self.h = CHUNK // 2
            self.first = wire.slots(26)
            self.whole = pl.ds(self.lo, CHUNK)
            self.spans = [pl.ds(self.lo, self.h), pl.ds(self.lo + self.h, self.h)]

        def expert_for(self, delta):
            return mine_expert if delta == 2 else 1 - mine_expert

        def gather_one(self):
            for i in range(self.lo, self.lo + CHUNK):
                if steps[i] != 0:
                    wire.arrived(bands.at[y, :, i], n_out + i, device(dz=-steps[i]))
            a, b = self.spans
            for way, delta in enumerate(ways):
                wire.send(
                    bands.at[y, self.expert_for(delta), a],
                    rows.at[y, x, c, a],
                    self.first + way,
                    device(dx=delta),
                )
                both = bands.at[y, pl.ds(0, 2), b]
                wire.send(both, both, self.first + 3 + way, device(dy=delta))
            rows[y, x, c, a] = bands[y, mine_expert, a]

        def gather_two(self):
            a, b = self.spans
            for way, delta in enumerate(ways):
                came_x = lax.rem(x - delta + 4, 4)
                wire.arrived(rows.at[y, came_x, c, a], self.first + way, device(dx=-delta))
            for way, delta in enumerate(ways):
                quad = rows.at[y, four, c, a]
                wire.send(quad, quad, self.first + 6 + way, device(dy=delta))
            for way, delta in enumerate(ways):
                came_y = lax.rem(y - delta + 4, 4)
                wire.arrived(
                    bands.at[came_y, pl.ds(0, 2), b], self.first + 3 + way, device(dy=-delta)
                )
            for way, delta in enumerate(ways):
                wire.send(
                    bands.at[four, self.expert_for(delta), b],
                    rows.at[four, x, c, b],
                    self.first + 9 + way,
                    device(dx=delta),
                )
            rows[four, x, c, b] = bands[four, mine_expert, b]

        def gather_three(self):
            a, b = self.spans
            for way, delta in enumerate(ways):
                came_x, came_y = lax.rem(x - delta + 4, 4), lax.rem(y - delta + 4, 4)
                wire.arrived(
                    rows.at[came_y, four, c, a], self.first + 6 + way, device(dy=-delta)
                )
                wire.arrived(
                    rows.at[four, came_x, c, b], self.first + 9 + way, device(dx=-delta)
                )
            mine = rows.at[four, four, c, self.whole]
            wire.send(mine, mine, self.first + 12, partner)

        def experts(self):
            wire.arrived(rows.at[four, four, 1 - c, self.whole], self.first + 12, partner)
            if self.lo == 0:
                weights_are_here()
            count = nc * CHUNK * cap
            squares = jnp.zeros((count, 128), F32)
            for t in range(tp):
                wide = rows[t // nx, t % nx, :, self.whole].astype(F32).reshape(count, 128)
                squares = squares + wide * wide
            scale = lax.rsqrt(jnp.sum(squares, axis=1, keepdims=True) / (tp * 128) + EPS)
            for t in range(tp):
                wide = rows[t // nx, t % nx, :, self.whole].astype(F32).reshape(count, 128)
                cols = slice(t * 128, (t + 1) * 128)
                normed[:, cols] = (wide * scale * row_gain[:, cols]).astype(BF)
            gate_acts = jnp.dot(normed[...], switch[...], preferred_element_type=F32)
            up_acts = jnp.dot(normed[...], raised[...], preferred_element_type=F32)
            hidden = (jax.nn.silu(gate_acts) * up_acts).astype(BF)
            for t in range(0, tp, 2):
                wide = jnp.dot(
                    hidden, lower[:, t * 128 : (t + 2) * 128], preferred_element_type=F32
                )
                for u in range(t, t + 2):
                    part[u // nx, u % nx, :, self.whole] = (
                        wide[:, (u - t) * 128 : (u - t + 1) * 128]
                        .reshape(nc, CHUNK, tiles, TILE, 128)
                        .astype(BF)
                    )
            wire.send(
                part.at[four, four, 1 - c, self.whole],
                other_part.at[four, four, self.whole],
                self.first + 13,
                partner,
            )

        def sum_one(self):
            came = other_part.at[four, four, self.whole]
            wire.arrived(came, self.first + 13, partner)
            for t in range(tp):
                at = (t // nx, t % nx)
                summed[at[0], at[1], self.whole] = (
                    part[at[0], at[1], c, self.whole].astype(F32)
                    + other_part[at[0], at[1], self.whole].astype(F32)
                ).astype(BF)
            a, b = self.spans
            for way, delta in enumerate(ways):
                to_y, to_x = lax.rem(y + delta + 4, 4), lax.rem(x + delta + 4, 4)
                wire.send(
                    summed.at[to_y, four, a],
                    red_one.at[way, four, a],
                    self.first + 14 + way,
                    device(dy=delta),
                )
                wire.send(
                    summed.at[four, to_x, b],
                    red_one.at[way, four, b],
                    self.first + 17 + way,
                    device(dx=delta),
                )

        def first_sum(self, index):
            a = self.spans[0]
            value = summed[y, index, a].astype(F32)
            for way in range(3):
                value = value + red_one[way, index, a].astype(F32)
            return value

        def second_sums(self, index):
            b = self.spans[1]
            own = summed[index, x, b].astype(F32) + red_one[0, index, b].astype(F32)
            return own, red_one[1, index, b].astype(F32) + red_one[2, index, b].astype(F32)

        def sum_two(self):
            a, b = self.spans
            for way, delta in enumerate(ways):
                wire.arrived(
                    red_one.at[way, four, a], self.first + 14 + way, device(dy=-delta)
                )
                wire.arrived(
                    red_one.at[way, four, b], self.first + 17 + way, device(dx=-delta)
                )
            red_a[four, a] = self.first_sum(four).astype(BF)
            own, other = self.second_sums(four)
            red_b[four, mine_expert, b] = own.astype(BF)
            red_b[four, 1 - mine_expert, b] = other.astype(BF)
            for way, delta in enumerate(ways):
                to_y, to_x = lax.rem(y + delta + 4, 4), lax.rem(x + delta + 4, 4)
                wire.send(
                    red_a.at[to_x, a],
                    last_a.at[way, a],
                    self.first + 20 + way,
                    device(dx=delta),
                )
                wire.send(
                    red_b.at[to_y, pl.ds(0, 2), b],
                    last_b.at[way, pl.ds(0, 2), b],
                    self.first + 23 + way,
                    device(dy=delta),
                )

        def give_back(self):
            a, b = self.spans
            for way, delta in enumerate(ways):
                wire.arrived(last_a.at[way, a], self.first + 20 + way, device(dx=-delta))
                wire.arrived(
                    last_b.at[way, pl.ds(0, 2), b], self.first + 23 + way, device(dy=-delta)
                )
            finished[mine_expert, a] = (
                self.first_sum(x) + last_a[0, a].astype(F32)
            ).astype(BF)
            finished[1 - mine_expert, a] = (
                last_a[1, a].astype(F32) + last_a[2, a].astype(F32)
            ).astype(BF)
            own, other = self.second_sums(y)
            for expert, value in ((mine_expert, own), (1 - mine_expert, other)):
                for way in range(3):
                    value = value + last_b[way, expert, b].astype(F32)
                finished[expert, b] = value.astype(BF)
            for i in range(self.lo, self.lo + CHUNK):
                if steps[i] == 0:
                    returned[pl.ds(2 * z, 2)] = finished[:, i]
                    continue
                wire.send(
                    finished.at[pl.ds(0, 2), i],
                    returned.at[pl.ds(2 * z, 2)],
                    n_home + i,
                    device(dz=-steps[i]),
                )

    n_home = wire.slots(nz)
    work = [Chunk(n) for n in range(chunks)]
    loads[12].wait()

    def weights_are_here():
        @pl.when(keeps)
        def _():
            for load in own_weights:
                load.wait()

        @pl.when(jnp.logical_not(keeps))
        def _():
            for copy in early + late:
                copy.wait_send()
                copy.wait_recv()

    order = (
        "gather_one",
        "gather_two",
        "gather_three",
        "experts",
        "sum_one",
        "sum_two",
        "give_back",
    )
    at = (0, 3, 7, 9, 11, 15, 19)
    tasks = sorted((at[j] + 2.2 * n, n, j) for n in range(chunks) for j in range(len(order)))
    for _, n, j in tasks:
        getattr(work[n], order[j])()

    for i, dz in enumerate(steps):
        if dz != 0:
            there = device(dz=dz)
            wire.arrived(returned.at[pl.ds(2 * there[0], 2)], n_home + i, there)
    got_rows = returned[...].astype(F32).reshape(experts * cap, 128).astype(BF)
    result = skip[...].astype(F32)
    for j in range(2):
        picked = jnp.dot(select_out[j], got_rows, preferred_element_type=F32)
        result = result + route[j] * picked
    out[...] = result.astype(BF)
    for copy in wire.started:
        copy.wait_send()


def layer(
    sizes,
    skip_path_vectors,
    asker_raw_scores,
    retain_raw_scores,
    memory_write_entries,
    emit_switch_scores,
    retain_minimum_share,
    extra_shrink_rate,
    lane_rescale_factor,
    emit_projection_array,
    specialist_rescale_factor,
    specialist_switch_proj,
    specialist_raise_proj,
    specialist_lower_proj,
    specialist_choice_ids,
    cluster_chance,
    specialist_duo_scores,
):
    nz, nc, ny, nx, tokens, cap = sizes
    tp = ny * nx
    width = tp * 128
    hidden = specialist_switch_proj.shape[2]
    half, experts, tiles = tokens // 2, nz * nc, cap // TILE
    block = (tiles, TILE, 128)
    vmem, anywhere = (
        pl.BlockSpec(memory_space=pltpu.VMEM),
        pl.BlockSpec(memory_space=pl.ANY),
    )
    count = semaphore_count(nz, nc, tp)
    scratch = [
        pltpu.VMEM((tokens, 128), BF),
        pltpu.VMEM((tokens, 128), BF),
        pltpu.VMEM((tokens, 128), BF),
        pltpu.VMEM((tokens, 128), BF),
        pltpu.VMEM((1, 128), F32),
        pltpu.VMEM((1, tokens), F32),
        pltpu.VMEM((1, 128), F32),
        pltpu.VMEM((1, width), F32),
        pltpu.VMEM((2, tokens), jnp.int32),
        pltpu.VMEM((1, tokens), F32),
        pltpu.VMEM((2, tokens), F32),
        pltpu.VMEM((tokens, 128), BF),
        pltpu.VMEM((128, width), BF),
        pltpu.VMEM((width, hidden), BF),
        pltpu.VMEM((width, hidden), BF),
        pltpu.VMEM((hidden, width), BF),
        pltpu.VMEM((width, hidden), BF),
        pltpu.VMEM((width, hidden), BF),
        pltpu.VMEM((hidden, width), BF),
        pltpu.VMEM((128, 128), F32),
        pltpu.VMEM((128, 128), F32),
        pltpu.VMEM((80, 128), BF),
        pltpu.VMEM((80, 128), BF),
        pltpu.VMEM((4, 80, 128), BF),
        pltpu.VMEM((nz // 4, 80, 128), BF),
        pltpu.VMEM((64, 128), BF),
        pltpu.VMEM((64, 128), BF),
        pltpu.VMEM((64, 128), F32),
        pltpu.VMEM((tokens, 128), F32),
        pltpu.VMEM((tokens, 128), F32),
        pltpu.VMEM((tokens, 128), F32),
        pltpu.VMEM((experts * cap, tokens), BF),
        pltpu.VMEM((2, tokens, experts * cap), BF),
        pltpu.VMEM((2, tokens, 128), F32),
        pltpu.VMEM((ny, nx, 2, 2, half // 2, 128), BF),
        pltpu.VMEM((2, 3, 4, 2, half // 2, 128), BF),
        pltpu.VMEM((2, 4, 2, half // 2, 128), BF),
        pltpu.VMEM((2, 3, 2, half // 2, 128), BF),
        pltpu.VMEM((experts, *block), BF),
        pltpu.VMEM((ny, 2, nz, *block), BF),
        pltpu.VMEM((ny, nx, nc, nz, *block), BF),
        pltpu.VMEM((nc * CHUNK * cap, width), BF),
        pltpu.VMEM((ny, nx, nc, nz, *block), BF),
        pltpu.VMEM((ny, nx, nz, *block), BF),
        pltpu.VMEM((ny, nx, nz, *block), BF),
        pltpu.VMEM((3, 4, nz, *block), BF),
        pltpu.VMEM((4, nz, *block), BF),
        pltpu.VMEM((4, 2, nz, *block), BF),
        pltpu.VMEM((3, nz, *block), BF),
        pltpu.VMEM((3, 2, nz, *block), BF),
        pltpu.VMEM((2, nz, *block), BF),
        pltpu.VMEM((experts, *block), BF),
        pltpu.SemaphoreType.DMA((19,)),
        pltpu.SemaphoreType.DMA((count,)),
        pltpu.SemaphoreType.DMA((count,)),
    ]
    return pl.pallas_call(
        functools.partial(kernel, sizes),
        out_shape=jax.ShapeDtypeStruct((tokens, 128), BF),
        in_specs=[anywhere] * 16,
        out_specs=vmem,
        scratch_shapes=scratch,
        compiler_params=pltpu.CompilerParams(collective_id=0, has_side_effects=True),
    )(
        asker_raw_scores,
        retain_raw_scores,
        memory_write_entries,
        emit_switch_scores,
        retain_minimum_share.reshape(1, 128),
        extra_shrink_rate,
        lane_rescale_factor.reshape(1, 128),
        specialist_rescale_factor.reshape(1, width),
        specialist_choice_ids.T,
        cluster_chance.reshape(1, tokens),
        specialist_duo_scores.T,
        skip_path_vectors,
        emit_projection_array,
        specialist_switch_proj[0],
        specialist_raise_proj[0],
        specialist_lower_proj[0],
    )


def solution(mesh, shape=(16, 2, 4, 4), tokens=256, cap=24):
    finer = Mesh(mesh.devices.reshape(shape), AXES)
    in_specs = (
        P(SP, None),
        P(SP, TP),
        P(SP, TP),
        P(SP, TP),
        P(SP, TP),
        P(TP),
        P(TP, SP),
        P(),
        P(TP, None),
        P(),
        P(SP, None, TP),
        P(SP, None, TP),
        P(SP, TP, None),
        P(SP, None),
        P(SP),
        P(SP, None),
    )
    return jax.shard_map(
        functools.partial(layer, (*shape, tokens, cap)),
        mesh=finer,
        in_specs=in_specs,
        out_specs=P(SP, TP),
        check_vma=False,
    )
```
